32 devices in a mesh: kv: 8 (over z, x), tp: 4 (over y, core).
Axes of the slice: x: 2, y: 2, z: 4, core: 2. Of those that a mesh axis runs over, the one named last changes fastest.
Arguments:
- hidden_in: bfloat16 [24, 4096], P('kv'), may hold values from -6 to 6
- norm_gain: float32 [4096], replicated, may hold values from 0.1 to 1.9
- w_query: bfloat16 [4096, 2048], P('kv', 'tp'), may hold values from -0.09375 to 0.09375
- w_key: bfloat16 [4096, 2048], P('kv', 'tp'), may hold values from -0.09375 to 0.09375
- w_value: bfloat16 [4096, 4096], P('kv', 'tp'), may hold values from -0.09375 to 0.09375
- w_out: bfloat16 [4096, 4096], P('kv', 'tp'), may hold values from -0.09375 to 0.09375
- carried_state: float32 [8, 8, 256, 512], P('kv', 'tp'), may hold values from -0.625 to 0.625
- prior_keys: bfloat16 [8, 8, 3, 256], P('kv', 'tp'), may hold values from -0.375 to 0.375
- prior_values: bfloat16 [8, 8, 3, 512], P('kv', 'tp'), may hold values from -6 to 6
- accepted: int32 [8], P('kv'), may hold values from 0 to 3
- lengths: int32 [8], P('kv'), may hold values from 1 to 4096
Outputs:
- layer_out: bfloat16 [24, 4096], P('tp', 'kv')
- committed_state: float32 [8, 8, 256, 512], P('kv', 'tp')
- new_keys: bfloat16 [8, 8, 3, 256], P('kv', 'tp')
- new_values: bfloat16 [8, 8, 3, 512], P('kv', 'tp')
The draws below stay inside these ranges and needn't reach their ends.
All inputs are finite; a program needn't handle non-finite values.
Results may differ from the reference program's by a relative error of at most 0.014.
Values may be sent and summed in bfloat16 or wider, within the bound.
A program may use at most 64 MiB of HBM per device.

```python
import jax
import jax.numpy as jnp
from jax import lax

D = 4096
HEADS = 8
DK = 256
DV = 512
PROPOSALS = 3
SEQS = 8
TOKENS = 24


def plant(entries, own_key, least, largest):
    shape = entries.shape
    place = [jax.random.randint(jax.random.fold_in(own_key, axis), (), 0, shape[axis]) for axis in range(len(shape))]
    entries = entries.at[tuple(place)].set(least)
    longest = shape.index(max(shape))
    place[longest] = (place[longest] + 1) % shape[longest]
    return entries.at[tuple(place)].set(largest)


def levels(rng, extent, shards, low, top_value):
    def one(dim, parts):
        heights = jax.random.uniform(jax.random.fold_in(jax.random.fold_in(rng, 6), dim), (parts,), jnp.float32, low / len(shards), top_value / len(shards))
        return jnp.repeat(jnp.exp(heights), extent[dim] // parts).reshape((-1,) + (1,) * (len(extent) - dim - 1))

    level = one(*shards[0])
    for cut in shards[1:]:
        level = level * one(*cut)
    return level


def noise(key, extent, spread, limit, cuts=(), kind=jnp.bfloat16):
    array = spread * jax.random.normal(key, extent, jnp.float32)
    if cuts:
        array = array * levels(key, extent, cuts, -0.22, 0.18)
    return jnp.clip(array, -limit, limit).astype(kind)


def setup_inputs(seed: int = 0) -> dict:
    splits = jax.random.split(jax.random.key(seed), 12)
    return {
        "hidden_in": noise(splits[0], (TOKENS, D), 1.0, 6.0, ((0, 8),)),
        "norm_gain": jnp.clip(1.0 + 0.18 * jax.random.normal(splits[1], (D,), jnp.float32), 0.1, 1.9),
        "w_query": noise(splits[2], (D, HEADS * DK), D ** -0.5, 0.09375, ((0, 8), (1, 4))),
        "w_key": noise(splits[3], (D, HEADS * DK), D ** -0.5, 0.09375, ((0, 8), (1, 4))),
        "w_value": noise(splits[4], (D, HEADS * DV), D ** -0.5, 0.09375, ((0, 8), (1, 4))),
        "w_out": noise(splits[5], (D, HEADS * DV), (HEADS * DV) ** -0.5, 0.09375, ((0, 8), (1, 4))),
        "carried_state": noise(splits[6], (SEQS, HEADS, DK, DV), 0.1, 0.625, ((0, 8), (1, 4)), jnp.float32),
        "prior_keys": noise(splits[7], (SEQS, HEADS, PROPOSALS, DK), 0.0625, 0.375, ((0, 8), (1, 4))),
        "prior_values": noise(splits[8], (SEQS, HEADS, PROPOSALS, DV), 1.0, 6.0, ((0, 8), (1, 4))),
        "accepted": plant(jax.random.randint(splits[9], (SEQS,), 0, PROPOSALS + 1), jax.random.fold_in(splits[9], 1), 0, PROPOSALS).astype(jnp.int32),
        "lengths": plant(jax.random.randint(splits[10], (SEQS,), 1, 4097), jax.random.fold_in(splits[10], 1), 1, 4096).astype(jnp.int32),
    }


epsilon = 1e-06
rotary_base = 10000.0

def rotate(values, places):
    middle = values.shape[-1] // 2
    inverse = rotary_base ** (-jnp.linspace(0.0, 1.0, middle, dtype=jnp.float32))
    angles = places[..., None] * inverse
    cosine = jnp.cos(angles)[:, :, None, :]
    sine_term = jnp.sin(angles)[:, :, None, :]
    leading = values[..., :middle]
    trailing = values[..., middle:]
    return jnp.concatenate([leading * cosine - trailing * sine_term, leading * sine_term + trailing * cosine], axis=-1)

def retain(queries, key_rows, value_rows, carried_state, prior_keys, prior_values, accepted, lengths, head_ids):
    steps_ahead = queries.shape[1]
    key_size = queries.shape[-1]
    log_decay = jnp.log(1.0 - 2.0 ** (-5.0 - head_ids))
    slot_ids = jnp.arange(steps_ahead, dtype=jnp.float32)
    places = (lengths + accepted).astype(jnp.float32)[:, None] + slot_ids[None, :]
    turned_q = rotate(queries.astype(jnp.float32), places)
    turned_k = rotate(key_rows.astype(jnp.float32), places) * key_size ** (-0.5)
    taken_count = accepted.astype(jnp.float32)[:, None]
    lag_steps = taken_count[:, :, None] - 1.0 - slot_ids[None, None, :]
    weights_back = jnp.where(lag_steps >= 0.0, jnp.exp(log_decay[None, :, None] * jnp.maximum(lag_steps, 0.0)), 0.0)
    keep_factor = jnp.exp(log_decay[None, :] * taken_count)
    scaled_keys = prior_keys.astype(jnp.float32) * weights_back[..., None]
    committed = keep_factor[..., None, None] * carried_state + jnp.einsum('shjd,shje->shde', scaled_keys, prior_values.astype(jnp.float32), precision=lax.Precision.HIGHEST)
    reach_decay = jnp.exp(log_decay[None, :] * (slot_ids[:, None] + 1.0))
    carried_part = jnp.einsum('sihd,shde->sihe', turned_q, committed, precision=lax.Precision.HIGHEST) * reach_decay[None, :, :, None]
    distance = slot_ids[:, None] - slot_ids[None, :]
    weight = jnp.where(distance[None] >= 0.0, jnp.exp(log_decay[:, None, None] * jnp.maximum(distance, 0.0)[None]), 0.0)
    scores = jnp.einsum('sihd,sjhd->shij', turned_q, turned_k, precision=lax.Precision.HIGHEST) * weight[None]
    inner_part = jnp.einsum('shij,sjhe->sihe', scores, value_rows.astype(jnp.float32), precision=lax.Precision.HIGHEST)
    retained = carried_part + inner_part
    normed = retained * lax.rsqrt(lax.optimization_barrier(jnp.mean(retained * retained, axis=-1, keepdims=True)) + epsilon)
    return (normed.astype(jnp.bfloat16), committed, turned_k)

def reference(hidden_in, norm_gain, w_query, w_key, w_value, w_out, carried_state, prior_keys, prior_values, accepted, lengths):
    row_values = hidden_in.astype(jnp.float32)
    normed = (row_values * lax.rsqrt(lax.optimization_barrier(jnp.mean(row_values * row_values, axis=-1, keepdims=True)) + epsilon) * norm_gain).astype(jnp.bfloat16)
    queries = jnp.dot(normed, w_query, preferred_element_type=jnp.float32).astype(jnp.bfloat16)
    key_rows = jnp.dot(normed, w_key, preferred_element_type=jnp.float32).astype(jnp.bfloat16)
    value_rows = jnp.dot(normed, w_value, preferred_element_type=jnp.float32).astype(jnp.bfloat16)
    sequences, head_count, steps_ahead = (prior_keys.shape[0], prior_keys.shape[1], prior_keys.shape[2])

    def by_heads(matrix):
        return matrix.reshape(sequences, steps_ahead, head_count, -1)
    head_ids = jnp.arange(head_count, dtype=jnp.float32)

    def one_sequence(packed):
        outs = retain(packed[0][None], packed[1][None], packed[2][None], packed[3][None], packed[4][None], packed[5][None], packed[6][None], packed[7][None], head_ids)
        return (outs[0][0], outs[1][0], outs[2][0])
    heads_out, committed, turned_k = lax.map(one_sequence, (by_heads(queries), by_heads(key_rows), by_heads(value_rows), carried_state, prior_keys, prior_values, accepted, lengths))
    flat_rows = heads_out.reshape(sequences * steps_ahead, -1)
    layer_out = lax.dot_general(flat_rows, w_out, (((1,), (1,)), ((), ())), preferred_element_type=jnp.float32).astype(jnp.bfloat16)
    new_keys = jnp.transpose(turned_k, (0, 2, 1, 3)).astype(jnp.bfloat16)
    new_values = jnp.transpose(by_heads(value_rows), (0, 2, 1, 3))
    return (layer_out, committed, new_keys, new_values)
```

```python
import functools

import jax
import jax.numpy as jnp
import numpy as np
from jax import lax
from jax.experimental import pallas as pl
from jax.experimental.pallas import tpu as pltpu
from jax.sharding import PartitionSpec as P

epsilon = 1e-06
rotary_base = 10000.0


def rotate(values, places):
    middle = values.shape[-1] // 2
    inverse = rotary_base ** (-jnp.linspace(0.0, 1.0, middle, dtype=jnp.float32))
    angles = places[..., None] * inverse
    cosine = jnp.cos(angles)[:, :, None, :]
    sine_term = jnp.sin(angles)[:, :, None, :]
    leading = values[..., :middle]
    trailing = values[..., middle:]
    return jnp.concatenate(
        [leading * cosine - trailing * sine_term, leading * sine_term + trailing * cosine], axis=-1
    )


def retain(
    queries,
    key_rows,
    value_rows,
    carried_state,
    prior_keys,
    prior_values,
    accepted,
    lengths,
    head_ids,
):
    steps_ahead = queries.shape[1]
    key_size = queries.shape[-1]
    log_decay = jnp.log(1.0 - 2.0 ** (-5.0 - head_ids))
    slot_ids = jnp.arange(steps_ahead, dtype=jnp.float32)
    places = (lengths + accepted).astype(jnp.float32)[:, None] + slot_ids[None, :]
    turned_q = rotate(queries.astype(jnp.float32), places)
    turned_k = rotate(key_rows.astype(jnp.float32), places) * key_size ** (-0.5)
    taken_count = accepted.astype(jnp.float32)[:, None]
    lag_steps = taken_count[:, :, None] - 1.0 - slot_ids[None, None, :]
    weights_back = jnp.where(
        lag_steps >= 0.0, jnp.exp(log_decay[None, :, None] * jnp.maximum(lag_steps, 0.0)), 0.0
    )
    keep_factor = jnp.exp(log_decay[None, :] * taken_count)
    scaled_keys = prior_keys.astype(jnp.float32) * weights_back[..., None]
    committed = keep_factor[..., None, None] * carried_state + jnp.einsum(
        "shjd,shje->shde",
        scaled_keys,
        prior_values.astype(jnp.float32),
        precision=lax.Precision.HIGHEST,
    )
    reach_decay = jnp.exp(log_decay[None, :] * (slot_ids[:, None] + 1.0))
    carried_part = (
        jnp.einsum("sihd,shde->sihe", turned_q, committed, precision=lax.Precision.HIGHEST)
        * reach_decay[None, :, :, None]
    )
    distance = slot_ids[:, None] - slot_ids[None, :]
    weight = jnp.where(
        distance[None] >= 0.0,
        jnp.exp(log_decay[:, None, None] * jnp.maximum(distance, 0.0)[None]),
        0.0,
    )
    scores = (
        jnp.einsum("sihd,sjhd->shij", turned_q, turned_k, precision=lax.Precision.HIGHEST)
        * weight[None]
    )
    inner_part = jnp.einsum(
        "shij,sjhe->sihe", scores, value_rows.astype(jnp.float32), precision=lax.Precision.HIGHEST
    )
    retained = carried_part + inner_part
    normed = retained * lax.rsqrt(jnp.mean(retained * retained, axis=-1, keepdims=True) + epsilon)
    return (normed.astype(jnp.bfloat16), committed, turned_k)


def body(
    hidden_in,
    norm_gain,
    w_query,
    w_key,
    w_value,
    w_out,
    carried_state,
    prior_keys,
    prior_values,
    accepted,
    lengths,
):
    row_values = hidden_in.astype(jnp.float32)
    normed = (
        row_values
        * lax.rsqrt(jnp.mean(row_values * row_values, axis=-1, keepdims=True) + epsilon)
        * norm_gain
    ).astype(jnp.bfloat16)
    own_rows = normed.shape[0]
    query_width = w_query.shape[1]
    key_width = w_key.shape[1]
    columns = lax.all_to_all(normed, "kv", split_axis=1, concat_axis=0, tiled=True)
    joined = jnp.concatenate((w_query, w_key, w_value), axis=1)
    group_count = lax.axis_size("kv")
    partial_term = jnp.dot(columns, joined, preferred_element_type=jnp.float32)
    grouped = partial_term.reshape(group_count, own_rows, partial_term.shape[1])
    received = lax.all_to_all(grouped, "kv", split_axis=0, concat_axis=0, tiled=True)
    joint_sum = jnp.sum(received, axis=0)
    query_sum = joint_sum[:, :query_width]
    key_sum = joint_sum[:, query_width : query_width + key_width]
    value_sum = joint_sum[:, query_width + key_width :]
    seq_count, head_count, steps_ahead = (
        prior_keys.shape[0],
        prior_keys.shape[1],
        prior_keys.shape[2],
    )

    def by_heads(matrix):
        return matrix.astype(jnp.bfloat16).reshape(seq_count, steps_ahead, head_count, -1)

    value_rows = by_heads(value_sum)
    head_ids = (lax.axis_index("tp") * head_count + jnp.arange(head_count)).astype(jnp.float32)
    heads_out, committed, turned_k = retain(
        by_heads(query_sum),
        by_heads(key_sum),
        value_rows,
        carried_state,
        prior_keys,
        prior_values,
        accepted,
        lengths,
        head_ids,
    )
    flat_rows = heads_out.reshape(own_rows, -1)
    head_terms = lax.dot_general(
        lax.all_gather(flat_rows, "kv", axis=0, tiled=True),
        w_out,
        (((1,), (1,)), ((), ())),
        preferred_element_type=jnp.float32,
    )
    layer_out = lax.psum_scatter(
        head_terms.astype(jnp.bfloat16), "tp", scatter_dimension=0, tiled=True
    )
    new_keys = jnp.transpose(turned_k, (0, 2, 1, 3)).astype(jnp.bfloat16)
    new_values = jnp.transpose(value_rows, (0, 2, 1, 3))
    return (layer_out, committed, new_keys, new_values)


MESH_ID = pl.DeviceIdType.MESH
SUB = 8
LANE = 128


def layer_kernel(
    kv_size,
    tp_size,
    hidden_hbm,
    gain_hbm,
    w_query_hbm,
    w_key_hbm,
    w_value_hbm,
    w_out_hbm,
    carried_hbm,
    prior_keys_hbm,
    prior_values_hbm,
    accepted_hbm,
    lengths_hbm,
    inverse_hbm,
    decay_hbm,
    layer_out_ref,
    committed_hbm,
    new_keys_hbm,
    new_values_hbm,
    hidden,
    gain,
    w_query,
    w_key,
    w_value,
    w_out,
    state,
    state_low,
    prior_keys,
    prior_values,
    accepted,
    lengths,
    inverse,
    decay,
    normed,
    own_keys,
    own_values,
    rows_recv,
    rows_pad,
    part_send_a,
    part_recv_a,
    part_send_b,
    part_recv_b,
    heads_all,
    heads_pad,
    out_send,
    out_recv,
    out_rows,
    load_sems,
    store_sems,
    a_send,
    a_recv,
    b_send,
    b_recv,
    c_send,
    c_recv,
    d_send,
    d_recv,
):
    me = lax.axis_index("kv")
    mine = lax.axis_index("tp")
    own_rows, width = hidden.shape
    block = width // kv_size
    head_count, key_size, value_size = state.shape[1:]
    half = key_size // 2
    key_width = head_count * key_size
    value_width = head_count * value_size
    per = kv_size // tp_size

    def kv_peer(d):
        return lax.rem(me + d, kv_size)

    def tp_peer(d):
        return lax.rem(mine + d, tp_size)

    barrier = pltpu.get_barrier_semaphore()
    for d in range(1, kv_size):
        pl.semaphore_signal(barrier, inc=1, device_id={"kv": kv_peer(d)}, device_id_type=MESH_ID)
    for d in range(1, tp_size):
        pl.semaphore_signal(barrier, inc=1, device_id={"tp": tp_peer(d)}, device_id_type=MESH_ID)

    pairs = (
        (hidden_hbm, hidden),
        (gain_hbm, gain),
        (accepted_hbm, accepted),
        (lengths_hbm, lengths),
        (inverse_hbm, inverse),
        (decay_hbm, decay),
        (prior_keys_hbm, prior_keys),
        (prior_values_hbm, prior_values),
        (carried_hbm, state),
        (w_query_hbm, w_query),
        (w_key_hbm, w_key),
        (w_value_hbm, w_value),
        (w_out_hbm, w_out),
    )
    loads = [pltpu.make_async_copy(s, t, load_sems.at[k]) for k, (s, t) in enumerate(pairs)]
    for load in loads:
        load.start()

    order = sorted(range(1, kv_size), key=lambda d: -min(d, kv_size - d))

    loads[0].wait()
    loads[1].wait()
    row_values = hidden[...].astype(jnp.float32)
    mean = jnp.mean(row_values * row_values, axis=-1, keepdims=True)
    normed[...] = (row_values * lax.rsqrt(mean + epsilon) * gain[...]).astype(jnp.bfloat16)
    rows_pad[...] = jnp.zeros_like(rows_pad)
    heads_pad[...] = jnp.zeros_like(heads_pad)

    pl.semaphore_wait(barrier, kv_size - 1 + tp_size - 1)

    sends = []
    waits_a = {}
    for d in order:
        copy = pltpu.make_async_remote_copy(
            src_ref=normed.at[:, pl.ds(pl.multiple_of(kv_peer(d) * block, LANE), block)],
            dst_ref=rows_recv.at[d],
            send_sem=a_send.at[d],
            recv_sem=a_recv.at[d],
            device_id={"kv": kv_peer(d)},
            device_id_type=MESH_ID,
        )
        copy.start()
        sends.append(copy)
        waits_a[d] = copy

    for load in loads[2:9]:
        load.wait()
    taken = accepted[0]
    start_place = lengths[0] + taken
    decays = []
    for h in range(head_count):
        g = decay[mine * head_count + h]
        powers = [jnp.float32(1.0)]
        for _ in range(own_rows):
            powers.append(powers[-1] * g)
        decays.append(powers)

    def power_of(powers, count):
        out = jnp.float32(0.0)
        for n, value in enumerate(powers):
            out = jnp.where(count == n, value, out)
        return out

    for h in range(head_count):
        powers = decays[h]
        keep = power_of(powers, taken)
        keys = prior_keys[0, h].astype(jnp.float32)
        values = prior_values[0, h].astype(jnp.float32)
        padded = jnp.concatenate([keys, jnp.zeros((SUB - own_rows, key_size), jnp.float32)], axis=0)
        columns = jnp.transpose(padded)
        total = keep * state[0, h]
        for j in range(own_rows):
            weight = power_of(powers, taken - 1 - j)
            total = total + (columns[:, j : j + 1] * weight) * values[j : j + 1, :]
        state[0, h] = total
        state_low[h] = total.astype(jnp.bfloat16)
    stores = [pltpu.make_async_copy(state, committed_hbm, store_sems.at[0])]
    stores[0].start()

    step_ids = lax.broadcasted_iota(jnp.int32, (own_rows, half), 0)
    angles = (step_ids + start_place).astype(jnp.float32) * inverse[...]
    cosine = jnp.cos(angles)
    sine = jnp.sin(angles)

    rows_pad[0:own_rows, :] = normed[:, pl.ds(pl.multiple_of(me * block, LANE), block)].astype(jnp.float32)
    for load in loads[9:12]:
        load.wait()
    for d in order:
        waits_a[d].wait_recv()
        rows_pad[SUB * d : SUB * d + own_rows, :] = rows_recv[d].astype(jnp.float32)
    stacked = rows_pad[...].astype(jnp.bfloat16)

    def send_parts(send_ref, recv_ref, chunk):
        made = []
        for d in order:
            e = kv_size - d
            copy = pltpu.make_async_remote_copy(
                src_ref=send_ref.at[d],
                dst_ref=recv_ref.at[e],
                send_sem=b_send.at[chunk, d],
                recv_sem=b_recv.at[chunk, e],
                device_id={"kv": kv_peer(e)},
                device_id_type=MESH_ID,
            )
            copy.start()
            made.append(copy)
        return made

    query_part = jnp.dot(stacked, w_query[...], preferred_element_type=jnp.float32)
    key_part = jnp.dot(stacked, w_key[...], preferred_element_type=jnp.float32)
    for d in range(kv_size):
        part_send_a[d, :, 0:key_width] = query_part[SUB * d : SUB * d + own_rows, :].astype(jnp.bfloat16)
        part_send_a[d, :, key_width:] = key_part[SUB * d : SUB * d + own_rows, :].astype(jnp.bfloat16)
    made_a = send_parts(part_send_a, part_recv_a, 0)
    value_part = jnp.dot(stacked, w_value[...], preferred_element_type=jnp.float32)
    for d in range(kv_size):
        part_send_b[d] = value_part[SUB * d : SUB * d + own_rows, :].astype(jnp.bfloat16)
    made_b = send_parts(part_send_b, part_recv_b, 1)
    sends += made_a + made_b

    joint = jnp.concatenate(
        [query_part[0:own_rows, :], key_part[0:own_rows, :]], axis=1
    )
    for copy in made_a:
        copy.wait_recv()
    for d in order:
        joint = joint + part_recv_a[d].astype(jnp.float32)
    joint = joint.astype(jnp.bfloat16).astype(jnp.float32)

    def turn(rows):
        leading = rows[:, :half]
        trailing = rows[:, half:]
        return jnp.concatenate(
            [leading * cosine - trailing * sine, leading * sine + trailing * cosine], axis=1
        )

    row_ids = lax.broadcasted_iota(jnp.int32, (own_rows, 1), 0)
    carried_parts = []
    score_columns = []
    for h in range(head_count):
        powers = decays[h]
        turned_q = turn(joint[:, h * key_size : (h + 1) * key_size])
        turned_k = turn(joint[:, key_width + h * key_size : key_width + (h + 1) * key_size])
        turned_k = turned_k * key_size ** (-0.5)
        own_keys[0, h] = turned_k.astype(jnp.bfloat16)
        reach = jnp.zeros((own_rows, 1), jnp.float32)
        for i in range(own_rows):
            reach = jnp.where(row_ids == i, powers[i + 1], reach)
        carried_parts.append(
            jnp.dot(turned_q.astype(jnp.bfloat16), state_low[h], preferred_element_type=jnp.float32)
            * reach
        )
        columns = []
        for j in range(own_rows):
            weight = jnp.zeros((own_rows, 1), jnp.float32)
            for i in range(j, own_rows):
                weight = jnp.where(row_ids == i, powers[i - j], weight)
            score = jnp.sum(turned_q * turned_k[j : j + 1, :], axis=-1, keepdims=True)
            columns.append(score * weight)
        score_columns.append(columns)
    stores.append(pltpu.make_async_copy(own_keys, new_keys_hbm, store_sems.at[1]))
    stores[1].start()

    value_rows = value_part[0:own_rows, :]
    for copy in made_b:
        copy.wait_recv()
    for d in order:
        value_rows = value_rows + part_recv_b[d].astype(jnp.float32)
    value_rows = value_rows.astype(jnp.bfloat16).astype(jnp.float32)
    head_rows = []
    for h in range(head_count):
        values = value_rows[:, h * value_size : (h + 1) * value_size]
        own_values[0, h] = values.astype(jnp.bfloat16)
        retained = carried_parts[h]
        for j in range(own_rows):
            retained = retained + score_columns[h][j] * values[j : j + 1, :]
        mean = jnp.mean(retained * retained, axis=-1, keepdims=True)
        head_rows.append(retained * lax.rsqrt(mean + epsilon))
    heads_all[me] = jnp.concatenate(head_rows, axis=1).astype(jnp.bfloat16)

    waits_c = []
    for d in order:
        copy = pltpu.make_async_remote_copy(
            src_ref=heads_all.at[me],
            dst_ref=heads_all.at[me],
            send_sem=c_send.at[d],
            recv_sem=c_recv.at[d],
            device_id={"kv": kv_peer(d)},
            device_id_type=MESH_ID,
        )
        copy.start()
        waits_c.append(copy)
    sends += waits_c
    stores.append(pltpu.make_async_copy(own_values, new_values_hbm, store_sems.at[2]))
    stores[2].start()
    loads[12].wait()
    for d in order:
        pltpu.make_async_remote_copy(
            src_ref=heads_all.at[me],
            dst_ref=heads_all.at[kv_peer(kv_size - d)],
            send_sem=c_send.at[d],
            recv_sem=c_recv.at[d],
            device_id={"kv": kv_peer(d)},
            device_id_type=MESH_ID,
        ).wait_recv()
    for j in range(kv_size):
        heads_pad[SUB * j : SUB * j + own_rows, :] = heads_all[j].astype(jnp.float32)
    terms = lax.dot_general(
        heads_pad[...].astype(jnp.bfloat16),
        w_out[...],
        (((1,), (1,)), ((), ())),
        preferred_element_type=jnp.float32,
    )
    for t in range(tp_size):
        for i in range(per):
            j = t * per + i
            out_send[t, i] = terms[SUB * j : SUB * j + own_rows, :].astype(jnp.bfloat16)
    waits_d = []
    for d in range(1, tp_size):
        copy = pltpu.make_async_remote_copy(
            src_ref=out_send.at[tp_peer(d)],
            dst_ref=out_recv.at[d],
            send_sem=d_send.at[d],
            recv_sem=d_recv.at[d],
            device_id={"tp": tp_peer(d)},
            device_id_type=MESH_ID,
        )
        copy.start()
        waits_d.append(copy)
    sends += waits_d
    own_terms = out_send[mine].astype(jnp.float32)
    for copy in waits_d:
        copy.wait_recv()
    for d in range(1, tp_size):
        own_terms = own_terms + out_recv[d].astype(jnp.float32)
    for i in range(per):
        out_rows[own_rows * i : own_rows * (i + 1), :] = own_terms[i]
    layer_out_ref[...] = out_rows[...].astype(jnp.bfloat16)
    for copy in sends:
        copy.wait_send()
    for store in stores:
        store.wait()


def fused_body(kv_size, tp_size, *args):
    hidden_in, norm_gain, w_query, w_key, w_value, w_out, carried_state = args[:7]
    prior_keys, prior_values, accepted, lengths = args[7:]
    own_rows, width = hidden_in.shape
    block = width // kv_size
    _, head_count, _, key_size = prior_keys.shape
    value_size = prior_values.shape[-1]
    half = key_size // 2
    heads = head_count * tp_size
    per = kv_size // tp_size
    inverse = (rotary_base ** (-np.linspace(0.0, 1.0, half))).astype(np.float32)[None, :]
    decay = (1.0 - 2.0 ** (-5.0 - np.arange(heads))).astype(np.float32)
    bf16, f32 = jnp.bfloat16, jnp.float32
    key_width = head_count * key_size
    value_width = head_count * value_size
    out_width = w_out.shape[0]
    any_spec = pl.BlockSpec(memory_space=pl.ANY)
    return pl.pallas_call(
        functools.partial(layer_kernel, kv_size, tp_size),
        out_shape=(
            jax.ShapeDtypeStruct((per * own_rows, out_width), bf16),
            jax.ShapeDtypeStruct(carried_state.shape, f32),
            jax.ShapeDtypeStruct(prior_keys.shape, bf16),
            jax.ShapeDtypeStruct(prior_values.shape, bf16),
        ),
        in_specs=[any_spec] * 13,
        out_specs=(pl.BlockSpec(memory_space=pltpu.VMEM), any_spec, any_spec, any_spec),
        scratch_shapes=[
            pltpu.VMEM(hidden_in.shape, bf16),
            pltpu.VMEM((1, width), f32),
            pltpu.VMEM(w_query.shape, bf16),
            pltpu.VMEM(w_key.shape, bf16),
            pltpu.VMEM(w_value.shape, bf16),
            pltpu.VMEM(w_out.shape, bf16),
            pltpu.VMEM(carried_state.shape, f32),
            pltpu.VMEM(carried_state.shape[1:], bf16),
            pltpu.VMEM(prior_keys.shape, bf16),
            pltpu.VMEM(prior_values.shape, bf16),
            pltpu.SMEM((1,), jnp.int32),
            pltpu.SMEM((1,), jnp.int32),
            pltpu.VMEM((1, half), f32),
            pltpu.SMEM((heads,), f32),
            pltpu.VMEM(hidden_in.shape, bf16),
            pltpu.VMEM(prior_keys.shape, bf16),
            pltpu.VMEM(prior_values.shape, bf16),
            pltpu.VMEM((kv_size, own_rows, block), bf16),
            pltpu.VMEM((kv_size * SUB, block), f32),
            pltpu.VMEM((kv_size, own_rows, 2 * key_width), bf16),
            pltpu.VMEM((kv_size, own_rows, 2 * key_width), bf16),
            pltpu.VMEM((kv_size, own_rows, value_width), bf16),
            pltpu.VMEM((kv_size, own_rows, value_width), bf16),
            pltpu.VMEM((kv_size, own_rows, value_width), bf16),
            pltpu.VMEM((kv_size * SUB, value_width), f32),
            pltpu.VMEM((tp_size, per, own_rows, out_width), bf16),
            pltpu.VMEM((tp_size, per, own_rows, out_width), bf16),
            pltpu.VMEM((per * own_rows, out_width), f32),
            pltpu.SemaphoreType.DMA((13,)),
            pltpu.SemaphoreType.DMA((3,)),
            pltpu.SemaphoreType.DMA((kv_size,)),
            pltpu.SemaphoreType.DMA((kv_size,)),
            pltpu.SemaphoreType.DMA((2, kv_size)),
            pltpu.SemaphoreType.DMA((2, kv_size)),
            pltpu.SemaphoreType.DMA((kv_size,)),
            pltpu.SemaphoreType.DMA((kv_size,)),
            pltpu.SemaphoreType.DMA((tp_size,)),
            pltpu.SemaphoreType.DMA((tp_size,)),
        ],
        compiler_params=pltpu.CompilerParams(collective_id=0, has_side_effects=True),
    )(
        hidden_in,
        norm_gain.reshape(1, width),
        w_query,
        w_key,
        w_value,
        w_out,
        carried_state,
        prior_keys,
        prior_values,
        accepted,
        lengths,
        inverse,
        decay,
    )


def kernel_fits(args):
    hidden_in, w_query, w_out, prior_keys = args[0], args[2], args[5], args[7]
    kv_size, tp_size = lax.axis_size("kv"), lax.axis_size("tp")
    return (
        prior_keys.shape[0] == 1
        and hidden_in.shape[0] == prior_keys.shape[2] <= SUB
        and w_query.shape[0] % LANE == 0
        and w_out.shape[0] % LANE == 0
        and prior_keys.shape[3] % (2 * LANE) == 0
        and kv_size % tp_size == 0
    )


def either(*args):
    if kernel_fits(args):
        return fused_body(lax.axis_size("kv"), lax.axis_size("tp"), *args)
    return body(*args)


def solution(mesh):
    in_specs = (
        P("kv", None),
        P(),
        P("kv", "tp"),
        P("kv", "tp"),
        P("kv", "tp"),
        P("kv", "tp"),
        P("kv", "tp", None, None),
        P("kv", "tp", None, None),
        P("kv", "tp", None, None),
        P("kv"),
        P("kv"),
    )
    out_specs = (
        P("tp", "kv"),
        P("kv", "tp", None, None),
        P("kv", "tp", None, None),
        P("kv", "tp", None, None),
    )
    return jax.shard_map(either, mesh=mesh, in_specs=in_specs, out_specs=out_specs, check_vma=False)
```

```python
import functools

import jax
import jax.numpy as jnp
import numpy as np
from jax import lax
from jax.experimental import pallas as pl
from jax.experimental.pallas import tpu as pltpu
from jax.sharding import PartitionSpec as P

epsilon = 1e-06
rotary_base = 10000.0


def rotate(values, places):
    middle = values.shape[-1] // 2
    inverse = rotary_base ** (-jnp.linspace(0.0, 1.0, middle, dtype=jnp.float32))
    angles = places[..., None] * inverse
    cosine = jnp.cos(angles)[:, :, None, :]
    sine_term = jnp.sin(angles)[:, :, None, :]
    leading = values[..., :middle]
    trailing = values[..., middle:]
    return jnp.concatenate(
        [leading * cosine - trailing * sine_term, leading * sine_term + trailing * cosine], axis=-1
    )


def retain(
    queries,
    key_rows,
    value_rows,
    carried_state,
    prior_keys,
    prior_values,
    accepted,
    lengths,
    head_ids,
):
    steps_ahead = queries.shape[1]
    key_size = queries.shape[-1]
    log_decay = jnp.log(1.0 - 2.0 ** (-5.0 - head_ids))
    slot_ids = jnp.arange(steps_ahead, dtype=jnp.float32)
    places = (lengths + accepted).astype(jnp.float32)[:, None] + slot_ids[None, :]
    turned_q = rotate(queries.astype(jnp.float32), places)
    turned_k = rotate(key_rows.astype(jnp.float32), places) * key_size ** (-0.5)
    taken_count = accepted.astype(jnp.float32)[:, None]
    lag_steps = taken_count[:, :, None] - 1.0 - slot_ids[None, None, :]
    weights_back = jnp.where(
        lag_steps >= 0.0, jnp.exp(log_decay[None, :, None] * jnp.maximum(lag_steps, 0.0)), 0.0
    )
    keep_factor = jnp.exp(log_decay[None, :] * taken_count)
    scaled_keys = prior_keys.astype(jnp.float32) * weights_back[..., None]
    committed = keep_factor[..., None, None] * carried_state + jnp.einsum(
        "shjd,shje->shde",
        scaled_keys,
        prior_values.astype(jnp.float32),
        precision=lax.Precision.HIGHEST,
    )
    reach_decay = jnp.exp(log_decay[None, :] * (slot_ids[:, None] + 1.0))
    carried_part = (
        jnp.einsum("sihd,shde->sihe", turned_q, committed, precision=lax.Precision.HIGHEST)
        * reach_decay[None, :, :, None]
    )
    distance = slot_ids[:, None] - slot_ids[None, :]
    weight = jnp.where(
        distance[None] >= 0.0,
        jnp.exp(log_decay[:, None, None] * jnp.maximum(distance, 0.0)[None]),
        0.0,
    )
    scores = (
        jnp.einsum("sihd,sjhd->shij", turned_q, turned_k, precision=lax.Precision.HIGHEST)
        * weight[None]
    )
    inner_part = jnp.einsum(
        "shij,sjhe->sihe", scores, value_rows.astype(jnp.float32), precision=lax.Precision.HIGHEST
    )
    retained = carried_part + inner_part
    normed = retained * lax.rsqrt(jnp.mean(retained * retained, axis=-1, keepdims=True) + epsilon)
    return (normed.astype(jnp.bfloat16), committed, turned_k)


def body(
    hidden_in,
    norm_gain,
    w_query,
    w_key,
    w_value,
    w_out,
    carried_state,
    prior_keys,
    prior_values,
    accepted,
    lengths,
):
    row_values = hidden_in.astype(jnp.float32)
    normed = (
        row_values
        * lax.rsqrt(jnp.mean(row_values * row_values, axis=-1, keepdims=True) + epsilon)
        * norm_gain
    ).astype(jnp.bfloat16)
    own_rows = normed.shape[0]
    query_width = w_query.shape[1]
    key_width = w_key.shape[1]
    columns = lax.all_to_all(normed, "kv", split_axis=1, concat_axis=0, tiled=True)
    joined = jnp.concatenate((w_query, w_key, w_value), axis=1)
    group_count = lax.axis_size("kv")
    partial_term = jnp.dot(columns, joined, preferred_element_type=jnp.float32)
    grouped = partial_term.reshape(group_count, own_rows, partial_term.shape[1])
    received = lax.all_to_all(grouped, "kv", split_axis=0, concat_axis=0, tiled=True)
    joint_sum = jnp.sum(received, axis=0)
    query_sum = joint_sum[:, :query_width]
    key_sum = joint_sum[:, query_width : query_width + key_width]
    value_sum = joint_sum[:, query_width + key_width :]
    seq_count, head_count, steps_ahead = (
        prior_keys.shape[0],
        prior_keys.shape[1],
        prior_keys.shape[2],
    )

    def by_heads(matrix):
        return matrix.astype(jnp.bfloat16).reshape(seq_count, steps_ahead, head_count, -1)

    value_rows = by_heads(value_sum)
    head_ids = (lax.axis_index("tp") * head_count + jnp.arange(head_count)).astype(jnp.float32)
    heads_out, committed, turned_k = retain(
        by_heads(query_sum),
        by_heads(key_sum),
        value_rows,
        carried_state,
        prior_keys,
        prior_values,
        accepted,
        lengths,
        head_ids,
    )
    flat_rows = heads_out.reshape(own_rows, -1)
    head_terms = lax.dot_general(
        lax.all_gather(flat_rows, "kv", axis=0, tiled=True),
        w_out,
        (((1,), (1,)), ((), ())),
        preferred_element_type=jnp.float32,
    )
    layer_out = lax.psum_scatter(
        head_terms.astype(jnp.bfloat16), "tp", scatter_dimension=0, tiled=True
    )
    new_keys = jnp.transpose(turned_k, (0, 2, 1, 3)).astype(jnp.bfloat16)
    new_values = jnp.transpose(value_rows, (0, 2, 1, 3))
    return (layer_out, committed, new_keys, new_values)


MESH_ID = pl.DeviceIdType.MESH
SUB = 8
LANE = 128


def layer_kernel(
    kv_size,
    tp_size,
    hidden_hbm,
    gain_hbm,
    w_query_hbm,
    w_key_hbm,
    w_value_hbm,
    w_out_hbm,
    carried_hbm,
    prior_keys_hbm,
    prior_values_hbm,
    accepted_hbm,
    lengths_hbm,
    inverse_hbm,
    decay_hbm,
    layer_out_ref,
    state,
    own_keys,
    own_values,
    hidden,
    gain,
    w_query,
    w_key,
    w_value,
    w_out,
    state_low,
    prior_keys,
    prior_values,
    accepted,
    lengths,
    inverse,
    decay,
    normed,
    rows_recv,
    rows_pad,
    part_send_a,
    part_recv_a,
    part_send_b,
    part_recv_b,
    heads_all,
    heads_pad,
    out_send,
    out_recv,
    out_rows,
    load_sems,
    a_send,
    a_recv,
    b_send,
    b_recv,
    c_send,
    c_recv,
    d_send,
    d_recv,
):
    me = lax.axis_index("kv")
    mine = lax.axis_index("tp")
    own_rows, width = hidden.shape
    block = width // kv_size
    head_count, key_size, value_size = state.shape[1:]
    half = key_size // 2
    key_width = head_count * key_size
    value_width = head_count * value_size
    per = kv_size // tp_size

    def kv_peer(d):
        return lax.rem(me + d, kv_size)

    def tp_peer(d):
        return lax.rem(mine + d, tp_size)

    barrier = pltpu.get_barrier_semaphore()
    for d in range(1, kv_size):
        pl.semaphore_signal(barrier, inc=1, device_id={"kv": kv_peer(d)}, device_id_type=MESH_ID)
    for d in range(1, tp_size):
        pl.semaphore_signal(barrier, inc=1, device_id={"tp": tp_peer(d)}, device_id_type=MESH_ID)

    pairs = (
        (hidden_hbm, hidden),
        (gain_hbm, gain),
        (accepted_hbm, accepted),
        (lengths_hbm, lengths),
        (inverse_hbm, inverse),
        (decay_hbm, decay),
        (prior_keys_hbm, prior_keys),
        (prior_values_hbm, prior_values),
        (carried_hbm, state),
        (w_query_hbm, w_query),
        (w_key_hbm, w_key),
        (w_value_hbm, w_value),
        (w_out_hbm, w_out),
    )
    loads = [pltpu.make_async_copy(s, t, load_sems.at[k]) for k, (s, t) in enumerate(pairs)]
    for load in loads:
        load.start()

    order = sorted(range(1, kv_size), key=lambda d: -min(d, kv_size - d))

    loads[0].wait()
    loads[1].wait()
    row_values = hidden[...].astype(jnp.float32)
    mean = jnp.mean(row_values * row_values, axis=-1, keepdims=True)
    normed[...] = (row_values * lax.rsqrt(mean + epsilon) * gain[...]).astype(jnp.bfloat16)
    rows_pad[...] = jnp.zeros_like(rows_pad)
    heads_pad[...] = jnp.zeros_like(heads_pad)

    pl.semaphore_wait(barrier, kv_size - 1 + tp_size - 1)

    sends = []
    waits_a = {}
    for d in order:
        copy = pltpu.make_async_remote_copy(
            src_ref=normed.at[:, pl.ds(pl.multiple_of(kv_peer(d) * block, LANE), block)],
            dst_ref=rows_recv.at[d],
            send_sem=a_send.at[d],
            recv_sem=a_recv.at[d],
            device_id={"kv": kv_peer(d)},
            device_id_type=MESH_ID,
        )
        copy.start()
        sends.append(copy)
        waits_a[d] = copy

    for load in loads[2:9]:
        load.wait()
    taken = accepted[0]
    start_place = lengths[0] + taken
    decays = []
    for h in range(head_count):
        g = decay[mine * head_count + h]
        powers = [jnp.float32(1.0)]
        for _ in range(own_rows):
            powers.append(powers[-1] * g)
        decays.append(powers)

    def power_of(powers, count):
        out = jnp.float32(0.0)
        for n, value in enumerate(powers):
            out = jnp.where(count == n, value, out)
        return out

    for h in range(head_count):
        powers = decays[h]
        keep = power_of(powers, taken)
        keys = prior_keys[0, :, h, :].astype(jnp.float32)
        values = prior_values[0, :, h, :].astype(jnp.float32)
        padded = jnp.concatenate([keys, jnp.zeros((SUB - own_rows, key_size), jnp.float32)], axis=0)
        columns = jnp.transpose(padded)
        total = keep * state[0, h]
        for j in range(own_rows):
            weight = power_of(powers, taken - 1 - j)
            total = total + (columns[:, j : j + 1] * weight) * values[j : j + 1, :]
        state[0, h] = total
        state_low[h] = total.astype(jnp.bfloat16)

    step_ids = lax.broadcasted_iota(jnp.int32, (own_rows, half), 0)
    angles = (step_ids + start_place).astype(jnp.float32) * inverse[...]
    cosine = jnp.cos(angles)
    sine = jnp.sin(angles)

    rows_pad[0:own_rows, :] = normed[:, pl.ds(pl.multiple_of(me * block, LANE), block)].astype(jnp.float32)
    for load in loads[9:12]:
        load.wait()
    for d in order:
        waits_a[d].wait_recv()
        rows_pad[SUB * d : SUB * d + own_rows, :] = rows_recv[d].astype(jnp.float32)
    stacked = rows_pad[...].astype(jnp.bfloat16)

    def send_parts(send_ref, recv_ref, chunk):
        made = []
        for d in order:
            e = kv_size - d
            copy = pltpu.make_async_remote_copy(
                src_ref=send_ref.at[d],
                dst_ref=recv_ref.at[e],
                send_sem=b_send.at[chunk, d],
                recv_sem=b_recv.at[chunk, e],
                device_id={"kv": kv_peer(e)},
                device_id_type=MESH_ID,
            )
            copy.start()
            made.append(copy)
        return made

    query_part = jnp.dot(stacked, w_query[...], preferred_element_type=jnp.float32)
    key_part = jnp.dot(stacked, w_key[...], preferred_element_type=jnp.float32)
    for d in range(kv_size):
        part_send_a[d, :, 0:key_width] = query_part[SUB * d : SUB * d + own_rows, :].astype(jnp.bfloat16)
        part_send_a[d, :, key_width:] = key_part[SUB * d : SUB * d + own_rows, :].astype(jnp.bfloat16)
    made_a = send_parts(part_send_a, part_recv_a, 0)
    value_part = jnp.dot(stacked, w_value[...], preferred_element_type=jnp.float32)
    for d in range(kv_size):
        part_send_b[d] = value_part[SUB * d : SUB * d + own_rows, :].astype(jnp.bfloat16)
    made_b = send_parts(part_send_b, part_recv_b, 1)
    sends += made_a + made_b

    joint = jnp.concatenate(
        [query_part[0:own_rows, :], key_part[0:own_rows, :]], axis=1
    )
    for copy in made_a:
        copy.wait_recv()
    for d in order:
        joint = joint + part_recv_a[d].astype(jnp.float32)
    joint = joint.astype(jnp.bfloat16).astype(jnp.float32)

    def turn(rows):
        leading = rows[:, :half]
        trailing = rows[:, half:]
        return jnp.concatenate(
            [leading * cosine - trailing * sine, leading * sine + trailing * cosine], axis=1
        )

    row_ids = lax.broadcasted_iota(jnp.int32, (own_rows, 1), 0)
    carried_parts = []
    score_columns = []
    for h in range(head_count):
        powers = decays[h]
        turned_q = turn(joint[:, h * key_size : (h + 1) * key_size])
        turned_k = turn(joint[:, key_width + h * key_size : key_width + (h + 1) * key_size])
        turned_k = turned_k * key_size ** (-0.5)
        own_keys[0, :, h, :] = turned_k.astype(jnp.bfloat16)
        reach = jnp.zeros((own_rows, 1), jnp.float32)
        for i in range(own_rows):
            reach = jnp.where(row_ids == i, powers[i + 1], reach)
        carried_parts.append(
            jnp.dot(turned_q.astype(jnp.bfloat16), state_low[h], preferred_element_type=jnp.float32)
            * reach
        )
        columns = []
        for j in range(own_rows):
            weight = jnp.zeros((own_rows, 1), jnp.float32)
            for i in range(j, own_rows):
                weight = jnp.where(row_ids == i, powers[i - j], weight)
            score = jnp.sum(turned_q * turned_k[j : j + 1, :], axis=-1, keepdims=True)
            columns.append(score * weight)
        score_columns.append(columns)

    value_rows = value_part[0:own_rows, :]
    for copy in made_b:
        copy.wait_recv()
    for d in order:
        value_rows = value_rows + part_recv_b[d].astype(jnp.float32)
    value_rows = value_rows.astype(jnp.bfloat16).astype(jnp.float32)
    head_rows = []
    for h in range(head_count):
        values = value_rows[:, h * value_size : (h + 1) * value_size]
        own_values[0, :, h, :] = values.astype(jnp.bfloat16)
        retained = carried_parts[h]
        for j in range(own_rows):
            retained = retained + score_columns[h][j] * values[j : j + 1, :]
        mean = jnp.mean(retained * retained, axis=-1, keepdims=True)
        head_rows.append(retained * lax.rsqrt(mean + epsilon))
    heads_all[me] = jnp.concatenate(head_rows, axis=1).astype(jnp.bfloat16)

    waits_c = []
    for d in order:
        copy = pltpu.make_async_remote_copy(
            src_ref=heads_all.at[me],
            dst_ref=heads_all.at[me],
            send_sem=c_send.at[d],
            recv_sem=c_recv.at[d],
            device_id={"kv": kv_peer(d)},
            device_id_type=MESH_ID,
        )
        copy.start()
        waits_c.append(copy)
    sends += waits_c
    loads[12].wait()
    for d in order:
        pltpu.make_async_remote_copy(
            src_ref=heads_all.at[me],
            dst_ref=heads_all.at[kv_peer(kv_size - d)],
            send_sem=c_send.at[d],
            recv_sem=c_recv.at[d],
            device_id={"kv": kv_peer(d)},
            device_id_type=MESH_ID,
        ).wait_recv()
    for j in range(kv_size):
        heads_pad[SUB * j : SUB * j + own_rows, :] = heads_all[j].astype(jnp.float32)
    terms = lax.dot_general(
        heads_pad[...].astype(jnp.bfloat16),
        w_out[...],
        (((1,), (1,)), ((), ())),
        preferred_element_type=jnp.float32,
    )
    for t in range(tp_size):
        for i in range(per):
            j = t * per + i
            out_send[t, i] = terms[SUB * j : SUB * j + own_rows, :].astype(jnp.bfloat16)
    waits_d = []
    for d in range(1, tp_size):
        copy = pltpu.make_async_remote_copy(
            src_ref=out_send.at[tp_peer(d)],
            dst_ref=out_recv.at[d],
            send_sem=d_send.at[d],
            recv_sem=d_recv.at[d],
            device_id={"tp": tp_peer(d)},
            device_id_type=MESH_ID,
        )
        copy.start()
        waits_d.append(copy)
    sends += waits_d
    own_terms = out_send[mine].astype(jnp.float32)
    for copy in waits_d:
        copy.wait_recv()
    for d in range(1, tp_size):
        own_terms = own_terms + out_recv[d].astype(jnp.float32)
    for i in range(per):
        out_rows[own_rows * i : own_rows * (i + 1), :] = own_terms[i]
    layer_out_ref[...] = out_rows[...].astype(jnp.bfloat16)
    for copy in sends:
        copy.wait_send()


def finish_kernel(*refs):
    sources, targets, sems = refs[:4], refs[4:8], refs[8]
    copies = [
        pltpu.make_async_copy(s, t, sems.at[k]) for k, (s, t) in enumerate(zip(sources, targets))
    ]
    for copy in reversed(copies):
        copy.start()
    for copy in copies:
        copy.wait()


def fused_body(kv_size, tp_size, *args):
    hidden_in, norm_gain, w_query, w_key, w_value, w_out, carried_state = args[:7]
    prior_keys, prior_values, accepted, lengths = args[7:]
    own_rows, width = hidden_in.shape
    block = width // kv_size
    _, head_count, _, key_size = prior_keys.shape
    prior_keys = jnp.transpose(prior_keys, (0, 2, 1, 3))
    prior_values = jnp.transpose(prior_values, (0, 2, 1, 3))
    value_size = prior_values.shape[-1]
    half = key_size // 2
    heads = head_count * tp_size
    per = kv_size // tp_size
    inverse = (rotary_base ** (-np.linspace(0.0, 1.0, half))).astype(np.float32)[None, :]
    decay = (1.0 - 2.0 ** (-5.0 - np.arange(heads))).astype(np.float32)
    bf16, f32 = jnp.bfloat16, jnp.float32
    key_width = head_count * key_size
    value_width = head_count * value_size
    out_width = w_out.shape[0]
    hbm_spec = pl.BlockSpec(memory_space=pltpu.HBM)
    vmem_spec = pl.BlockSpec(memory_space=pltpu.VMEM)
    results = pl.pallas_call(
        functools.partial(layer_kernel, kv_size, tp_size),
        out_shape=(
            pltpu.VMEM((per * own_rows, out_width), bf16),
            pltpu.VMEM(carried_state.shape, f32),
            pltpu.VMEM(prior_keys.shape, bf16),
            pltpu.VMEM(prior_values.shape, bf16),
        ),
        in_specs=[hbm_spec] * 13,
        out_specs=(vmem_spec,) * 4,
        scratch_shapes=[
            pltpu.VMEM(hidden_in.shape, bf16),
            pltpu.VMEM((1, width), f32),
            pltpu.VMEM(w_query.shape, bf16),
            pltpu.VMEM(w_key.shape, bf16),
            pltpu.VMEM(w_value.shape, bf16),
            pltpu.VMEM(w_out.shape, bf16),
            pltpu.VMEM(carried_state.shape[1:], bf16),
            pltpu.VMEM(prior_keys.shape, bf16),
            pltpu.VMEM(prior_values.shape, bf16),
            pltpu.SMEM((1,), jnp.int32),
            pltpu.SMEM((1,), jnp.int32),
            pltpu.VMEM((1, half), f32),
            pltpu.SMEM((heads,), f32),
            pltpu.VMEM(hidden_in.shape, bf16),
            pltpu.VMEM((kv_size, own_rows, block), bf16),
            pltpu.VMEM((kv_size * SUB, block), f32),
            pltpu.VMEM((kv_size, own_rows, 2 * key_width), bf16),
            pltpu.VMEM((kv_size, own_rows, 2 * key_width), bf16),
            pltpu.VMEM((kv_size, own_rows, value_width), bf16),
            pltpu.VMEM((kv_size, own_rows, value_width), bf16),
            pltpu.VMEM((kv_size, own_rows, value_width), bf16),
            pltpu.VMEM((kv_size * SUB, value_width), f32),
            pltpu.VMEM((tp_size, per, own_rows, out_width), bf16),
            pltpu.VMEM((tp_size, per, own_rows, out_width), bf16),
            pltpu.VMEM((per * own_rows, out_width), f32),
            pltpu.SemaphoreType.DMA((13,)),
            pltpu.SemaphoreType.DMA((kv_size,)),
            pltpu.SemaphoreType.DMA((kv_size,)),
            pltpu.SemaphoreType.DMA((2, kv_size)),
            pltpu.SemaphoreType.DMA((2, kv_size)),
            pltpu.SemaphoreType.DMA((kv_size,)),
            pltpu.SemaphoreType.DMA((kv_size,)),
            pltpu.SemaphoreType.DMA((tp_size,)),
            pltpu.SemaphoreType.DMA((tp_size,)),
        ],
        compiler_params=pltpu.CompilerParams(collective_id=0, has_side_effects=True),
    )(
        hidden_in,
        norm_gain.reshape(1, width),
        w_query,
        w_key,
        w_value,
        w_out,
        carried_state,
        prior_keys,
        prior_values,
        accepted,
        lengths,
        inverse,
        decay,
    )
    layer_out, committed, new_keys, new_values = pl.pallas_call(
        finish_kernel,
        out_shape=tuple(jax.ShapeDtypeStruct(r.shape, r.dtype) for r in results),
        in_specs=[vmem_spec] * 4,
        out_specs=(hbm_spec,) * 4,
        scratch_shapes=[pltpu.SemaphoreType.DMA((4,))],
    )(*[pltpu.with_memory_space_constraint(r, pltpu.VMEM) for r in results])
    return (
        layer_out,
        committed,
        jnp.transpose(new_keys, (0, 2, 1, 3)),
        jnp.transpose(new_values, (0, 2, 1, 3)),
    )


def kernel_fits(args):
    hidden_in, w_query, w_out, prior_keys = args[0], args[2], args[5], args[7]
    kv_size, tp_size = lax.axis_size("kv"), lax.axis_size("tp")
    return (
        prior_keys.shape[0] == 1
        and hidden_in.shape[0] == prior_keys.shape[2] <= SUB
        and w_query.shape[0] % LANE == 0
        and w_out.shape[0] % LANE == 0
        and prior_keys.shape[3] % (2 * LANE) == 0
        and kv_size % tp_size == 0
    )


def either(*args):
    if kernel_fits(args):
        return fused_body(lax.axis_size("kv"), lax.axis_size("tp"), *args)
    return body(*args)


def solution(mesh):
    in_specs = (
        P("kv", None),
        P(),
        P("kv", "tp"),
        P("kv", "tp"),
        P("kv", "tp"),
        P("kv", "tp"),
        P("kv", "tp", None, None),
        P("kv", "tp", None, None),
        P("kv", "tp", None, None),
        P("kv"),
        P("kv"),
    )
    out_specs = (
        P("tp", "kv"),
        P("kv", "tp", None, None),
        P("kv", "tp", None, None),
        P("kv", "tp", None, None),
    )
    return jax.shard_map(either, mesh=mesh, in_specs=in_specs, out_specs=out_specs, check_vma=False)
```

```python
import functools

import jax
import jax.numpy as jnp
import numpy as np
from jax import lax
from jax.experimental import pallas as pl
from jax.experimental.pallas import tpu as pltpu
from jax.sharding import PartitionSpec as P

epsilon = 1e-06
rotary_base = 10000.0


def rotate(values, places):
    middle = values.shape[-1] // 2
    inverse = rotary_base ** (-jnp.linspace(0.0, 1.0, middle, dtype=jnp.float32))
    angles = places[..., None] * inverse
    cosine = jnp.cos(angles)[:, :, None, :]
    sine_term = jnp.sin(angles)[:, :, None, :]
    leading = values[..., :middle]
    trailing = values[..., middle:]
    return jnp.concatenate(
        [leading * cosine - trailing * sine_term, leading * sine_term + trailing * cosine], axis=-1
    )


def retain(
    queries,
    key_rows,
    value_rows,
    carried_state,
    prior_keys,
    prior_values,
    accepted,
    lengths,
    head_ids,
):
    steps_ahead = queries.shape[1]
    key_size = queries.shape[-1]
    log_decay = jnp.log(1.0 - 2.0 ** (-5.0 - head_ids))
    slot_ids = jnp.arange(steps_ahead, dtype=jnp.float32)
    places = (lengths + accepted).astype(jnp.float32)[:, None] + slot_ids[None, :]
    turned_q = rotate(queries.astype(jnp.float32), places)
    turned_k = rotate(key_rows.astype(jnp.float32), places) * key_size ** (-0.5)
    taken_count = accepted.astype(jnp.float32)[:, None]
    lag_steps = taken_count[:, :, None] - 1.0 - slot_ids[None, None, :]
    weights_back = jnp.where(
        lag_steps >= 0.0, jnp.exp(log_decay[None, :, None] * jnp.maximum(lag_steps, 0.0)), 0.0
    )
    keep_factor = jnp.exp(log_decay[None, :] * taken_count)
    scaled_keys = prior_keys.astype(jnp.float32) * weights_back[..., None]
    committed = keep_factor[..., None, None] * carried_state + jnp.einsum(
        "shjd,shje->shde",
        scaled_keys,
        prior_values.astype(jnp.float32),
        precision=lax.Precision.HIGHEST,
    )
    reach_decay = jnp.exp(log_decay[None, :] * (slot_ids[:, None] + 1.0))
    carried_part = (
        jnp.einsum("sihd,shde->sihe", turned_q, committed, precision=lax.Precision.HIGHEST)
        * reach_decay[None, :, :, None]
    )
    distance = slot_ids[:, None] - slot_ids[None, :]
    weight = jnp.where(
        distance[None] >= 0.0,
        jnp.exp(log_decay[:, None, None] * jnp.maximum(distance, 0.0)[None]),
        0.0,
    )
    scores = (
        jnp.einsum("sihd,sjhd->shij", turned_q, turned_k, precision=lax.Precision.HIGHEST)
        * weight[None]
    )
    inner_part = jnp.einsum(
        "shij,sjhe->sihe", scores, value_rows.astype(jnp.float32), precision=lax.Precision.HIGHEST
    )
    retained = carried_part + inner_part
    normed = retained * lax.rsqrt(jnp.mean(retained * retained, axis=-1, keepdims=True) + epsilon)
    return (normed.astype(jnp.bfloat16), committed, turned_k)


def body(
    hidden_in,
    norm_gain,
    w_query,
    w_key,
    w_value,
    w_out,
    carried_state,
    prior_keys,
    prior_values,
    accepted,
    lengths,
):
    row_values = hidden_in.astype(jnp.float32)
    normed = (
        row_values
        * lax.rsqrt(jnp.mean(row_values * row_values, axis=-1, keepdims=True) + epsilon)
        * norm_gain
    ).astype(jnp.bfloat16)
    own_rows = normed.shape[0]
    query_width = w_query.shape[1]
    key_width = w_key.shape[1]
    columns = lax.all_to_all(normed, "kv", split_axis=1, concat_axis=0, tiled=True)
    joined = jnp.concatenate((w_query, w_key, w_value), axis=1)
    group_count = lax.axis_size("kv")
    partial_term = jnp.dot(columns, joined, preferred_element_type=jnp.float32)
    grouped = partial_term.reshape(group_count, own_rows, partial_term.shape[1])
    received = lax.all_to_all(grouped, "kv", split_axis=0, concat_axis=0, tiled=True)
    joint_sum = jnp.sum(received, axis=0)
    query_sum = joint_sum[:, :query_width]
    key_sum = joint_sum[:, query_width : query_width + key_width]
    value_sum = joint_sum[:, query_width + key_width :]
    seq_count, head_count, steps_ahead = (
        prior_keys.shape[0],
        prior_keys.shape[1],
        prior_keys.shape[2],
    )

    def by_heads(matrix):
        return matrix.astype(jnp.bfloat16).reshape(seq_count, steps_ahead, head_count, -1)

    value_rows = by_heads(value_sum)
    head_ids = (lax.axis_index("tp") * head_count + jnp.arange(head_count)).astype(jnp.float32)
    heads_out, committed, turned_k = retain(
        by_heads(query_sum),
        by_heads(key_sum),
        value_rows,
        carried_state,
        prior_keys,
        prior_values,
        accepted,
        lengths,
        head_ids,
    )
    flat_rows = heads_out.reshape(own_rows, -1)
    head_terms = lax.dot_general(
        lax.all_gather(flat_rows, "kv", axis=0, tiled=True),
        w_out,
        (((1,), (1,)), ((), ())),
        preferred_element_type=jnp.float32,
    )
    layer_out = lax.psum_scatter(
        head_terms.astype(jnp.bfloat16), "tp", scatter_dimension=0, tiled=True
    )
    new_keys = jnp.transpose(turned_k, (0, 2, 1, 3)).astype(jnp.bfloat16)
    new_values = jnp.transpose(value_rows, (0, 2, 1, 3))
    return (layer_out, committed, new_keys, new_values)


MESH_ID = pl.DeviceIdType.MESH
SUB = 8
LANE = 128


def layer_kernel(
    kv_size,
    tp_size,
    hidden_hbm,
    gain_hbm,
    w_query_hbm,
    w_key_hbm,
    w_value_hbm,
    w_out_hbm,
    carried_hbm,
    prior_keys_hbm,
    prior_values_hbm,
    accepted_hbm,
    lengths_hbm,
    inverse_hbm,
    decay_hbm,
    layer_out_ref,
    state,
    own_keys,
    own_values,
    hidden,
    gain,
    w_query,
    w_key,
    w_value,
    w_out,
    state_low,
    prior_keys,
    prior_values,
    inverse,
    decay,
    normed,
    rows_recv,
    rows_pad,
    part_send_a,
    part_recv_a,
    part_send_b,
    part_recv_b,
    packed,
    summed_a,
    summed_b,
    heads_all,
    heads_pad,
    out_send,
    out_recv,
    out_rows,
    load_sems,
    a_send,
    a_recv,
    b_send,
    b_recv,
    c_send,
    c_recv,
    d_send,
    d_recv,
):
    me = lax.axis_index("kv")
    mine = lax.axis_index("tp")
    own_rows, width = hidden.shape
    block = width // kv_size
    head_count, key_size, value_size = state.shape[1:]
    half = key_size // 2
    key_width = head_count * key_size
    value_width = head_count * value_size
    per = kv_size // tp_size

    def kv_peer(d):
        return lax.rem(me + d, kv_size)

    def tp_peer(d):
        return lax.rem(mine + d, tp_size)

    barrier = pltpu.get_barrier_semaphore()
    for d in range(1, kv_size):
        pl.semaphore_signal(barrier, inc=1, device_id={"kv": kv_peer(d)}, device_id_type=MESH_ID)
    for d in range(1, tp_size):
        pl.semaphore_signal(barrier, inc=1, device_id={"tp": tp_peer(d)}, device_id_type=MESH_ID)

    pairs = (
        (hidden_hbm, hidden),
        (gain_hbm, gain),
        (inverse_hbm, inverse),
        (decay_hbm, decay),
        (prior_keys_hbm, prior_keys),
        (prior_values_hbm, prior_values),
        (carried_hbm, state),
        (w_query_hbm, w_query),
        (w_key_hbm, w_key),
        (w_value_hbm, w_value),
        (w_out_hbm, w_out),
    )
    loads = [pltpu.make_async_copy(s, t, load_sems.at[k]) for k, (s, t) in enumerate(pairs)]
    for load in loads:
        load.start()

    order = sorted(range(1, kv_size), key=lambda d: -min(d, kv_size - d))

    loads[0].wait()
    loads[1].wait()
    row_values = hidden[...].astype(jnp.float32)
    mean = jnp.mean(row_values * row_values, axis=-1, keepdims=True)
    normed[...] = (row_values * lax.rsqrt(mean + epsilon) * gain[...]).astype(jnp.bfloat16)
    rows_pad[...] = jnp.zeros_like(rows_pad)
    heads_pad[...] = jnp.zeros_like(heads_pad)

    pl.semaphore_wait(barrier, kv_size - 1 + tp_size - 1)

    sends = []
    waits_a = {}
    for d in order:
        copy = pltpu.make_async_remote_copy(
            src_ref=normed.at[:, pl.ds(pl.multiple_of(kv_peer(d) * block, LANE), block)],
            dst_ref=rows_recv.at[d],
            send_sem=a_send.at[d],
            recv_sem=a_recv.at[d],
            device_id={"kv": kv_peer(d)},
            device_id_type=MESH_ID,
        )
        copy.start()
        sends.append(copy)
        waits_a[d] = copy

    for load in loads[2:7]:
        load.wait()
    taken = jnp.full((1, 1), accepted_hbm[0], jnp.int32)
    start_place = lengths_hbm[0] + taken
    decays = []
    for h in range(head_count):
        g = decay[mine * head_count + h]
        powers = [jnp.float32(1.0)]
        for _ in range(own_rows):
            powers.append(powers[-1] * g)
        decays.append(powers)

    def power_of(powers, count):
        out = jnp.zeros(count.shape, jnp.float32)
        for n, value in enumerate(powers):
            out = jnp.where(count == n, value, out)
        return out

    for h in range(head_count):
        powers = decays[h]
        keep = power_of(powers, taken)
        keys = prior_keys[0, :, h, :].astype(jnp.float32)
        values = prior_values[0, :, h, :].astype(jnp.float32)
        padded = jnp.concatenate([keys, jnp.zeros((SUB - own_rows, key_size), jnp.float32)], axis=0)
        columns = jnp.transpose(padded)
        total = keep * state[0, h]
        for j in range(own_rows):
            weight = power_of(powers, taken - 1 - j)
            total = total + (columns[:, j : j + 1] * weight) * values[j : j + 1, :]
        state[0, h] = total
        state_low[h] = total.astype(jnp.bfloat16)

    step_ids = lax.broadcasted_iota(jnp.int32, (own_rows, half), 0)
    angles = (step_ids + start_place).astype(jnp.float32) * inverse[...]
    cosine = jnp.cos(angles)
    sine = jnp.sin(angles)

    rows_pad[0:own_rows, :] = normed[:, pl.ds(pl.multiple_of(me * block, LANE), block)].astype(jnp.float32)
    for load in loads[7:10]:
        load.wait()
    for d in order:
        waits_a[d].wait_recv()
        rows_pad[SUB * d : SUB * d + own_rows, :] = rows_recv[d].astype(jnp.float32)
    stacked = rows_pad[...].astype(jnp.bfloat16)

    def pack(part, first):
        for d in range(kv_size):
            for g in range(part.shape[1] // LANE):
                low = (first + g) * own_rows
                packed[d, low : low + own_rows, :] = part[
                    SUB * d : SUB * d + own_rows, g * LANE : (g + 1) * LANE
                ]

    def send_parts(send_ref, recv_ref, chunk):
        made = []
        for d in order:
            e = kv_size - d
            copy = pltpu.make_async_remote_copy(
                src_ref=send_ref.at[d],
                dst_ref=recv_ref.at[e],
                send_sem=b_send.at[chunk, d],
                recv_sem=b_recv.at[chunk, e],
                device_id={"kv": kv_peer(e)},
                device_id_type=MESH_ID,
            )
            copy.start()
            made.append(copy)
        return made

    query_part = jnp.dot(stacked, w_query[...], preferred_element_type=jnp.float32)
    key_part = jnp.dot(stacked, w_key[...], preferred_element_type=jnp.float32)
    pack(query_part, 0)
    pack(key_part, key_width // LANE)
    part_send_a[...] = packed[:, : part_send_a.shape[1], :].astype(jnp.bfloat16)
    made_a = send_parts(part_send_a, part_recv_a, 0)
    value_part = jnp.dot(stacked, w_value[...], preferred_element_type=jnp.float32)
    own_a = packed[0, : part_send_a.shape[1], :]
    pack(value_part, 0)
    part_send_b[...] = packed[:, : part_send_b.shape[1], :].astype(jnp.bfloat16)
    made_b = send_parts(part_send_b, part_recv_b, 1)
    sends += made_a + made_b

    joint = own_a
    for copy in made_a:
        copy.wait_recv()
    for d in order:
        joint = joint + part_recv_a[d].astype(jnp.float32)
    summed_a[...] = joint.astype(jnp.bfloat16).astype(jnp.float32)

    def unpack(ref, column, size):
        low = column // LANE
        return jnp.concatenate(
            [ref[g * own_rows : (g + 1) * own_rows, :] for g in range(low, low + size // LANE)], axis=1
        )

    def turn(rows):
        leading = rows[:, :half]
        trailing = rows[:, half:]
        return jnp.concatenate(
            [leading * cosine - trailing * sine, leading * sine + trailing * cosine], axis=1
        )

    row_ids = lax.broadcasted_iota(jnp.int32, (own_rows, 1), 0)
    carried_parts = []
    score_columns = []
    for h in range(head_count):
        powers = decays[h]
        turned_q = turn(unpack(summed_a, h * key_size, key_size))
        turned_k = turn(unpack(summed_a, key_width + h * key_size, key_size))
        turned_k = turned_k * key_size ** (-0.5)
        own_keys[0, :, h, :] = turned_k.astype(jnp.bfloat16)
        reach = jnp.zeros((own_rows, 1), jnp.float32)
        for i in range(own_rows):
            reach = jnp.where(row_ids == i, powers[i + 1], reach)
        carried_parts.append(
            jnp.dot(turned_q.astype(jnp.bfloat16), state_low[h], preferred_element_type=jnp.float32)
            * reach
        )
        columns = []
        for j in range(own_rows):
            weight = jnp.zeros((own_rows, 1), jnp.float32)
            for i in range(j, own_rows):
                weight = jnp.where(row_ids == i, powers[i - j], weight)
            score = jnp.sum(turned_q * turned_k[j : j + 1, :], axis=-1, keepdims=True)
            columns.append(score * weight)
        score_columns.append(columns)

    value_rows = packed[0, : part_send_b.shape[1], :]
    for copy in made_b:
        copy.wait_recv()
    for d in order:
        value_rows = value_rows + part_recv_b[d].astype(jnp.float32)
    summed_b[...] = value_rows.astype(jnp.bfloat16).astype(jnp.float32)
    head_rows = []
    for h in range(head_count):
        values = unpack(summed_b, h * value_size, value_size)
        own_values[0, :, h, :] = values.astype(jnp.bfloat16)
        retained = carried_parts[h]
        for j in range(own_rows):
            retained = retained + score_columns[h][j] * values[j : j + 1, :]
        mean = jnp.mean(retained * retained, axis=-1, keepdims=True)
        head_rows.append(retained * lax.rsqrt(mean + epsilon))
    heads_all[me] = jnp.concatenate(head_rows, axis=1).astype(jnp.bfloat16)

    waits_c = []
    for d in order:
        copy = pltpu.make_async_remote_copy(
            src_ref=heads_all.at[me],
            dst_ref=heads_all.at[me],
            send_sem=c_send.at[d],
            recv_sem=c_recv.at[d],
            device_id={"kv": kv_peer(d)},
            device_id_type=MESH_ID,
        )
        copy.start()
        waits_c.append(copy)
    sends += waits_c
    loads[10].wait()
    for d in order:
        pltpu.make_async_remote_copy(
            src_ref=heads_all.at[me],
            dst_ref=heads_all.at[kv_peer(kv_size - d)],
            send_sem=c_send.at[d],
            recv_sem=c_recv.at[d],
            device_id={"kv": kv_peer(d)},
            device_id_type=MESH_ID,
        ).wait_recv()
    for j in range(kv_size):
        heads_pad[SUB * j : SUB * j + own_rows, :] = heads_all[j].astype(jnp.float32)
    terms = lax.dot_general(
        heads_pad[...].astype(jnp.bfloat16),
        w_out[...],
        (((1,), (1,)), ((), ())),
        preferred_element_type=jnp.float32,
    )
    for t in range(tp_size):
        for i in range(per):
            j = t * per + i
            out_send[t, i] = terms[SUB * j : SUB * j + own_rows, :].astype(jnp.bfloat16)
    waits_d = []
    for d in range(1, tp_size):
        copy = pltpu.make_async_remote_copy(
            src_ref=out_send.at[tp_peer(d)],
            dst_ref=out_recv.at[d],
            send_sem=d_send.at[d],
            recv_sem=d_recv.at[d],
            device_id={"tp": tp_peer(d)},
            device_id_type=MESH_ID,
        )
        copy.start()
        waits_d.append(copy)
    sends += waits_d
    own_terms = out_send[mine].astype(jnp.float32)
    for copy in waits_d:
        copy.wait_recv()
    for d in range(1, tp_size):
        own_terms = own_terms + out_recv[d].astype(jnp.float32)
    for i in range(per):
        out_rows[own_rows * i : own_rows * (i + 1), :] = own_terms[i]
    layer_out_ref[...] = out_rows[...].astype(jnp.bfloat16)
    for copy in sends:
        copy.wait_send()


def finish_kernel(*refs):
    sources, targets, sems = refs[:4], refs[4:8], refs[8]
    copies = [
        pltpu.make_async_copy(s, t, sems.at[k]) for k, (s, t) in enumerate(zip(sources, targets))
    ]
    for copy in reversed(copies):
        copy.start()
    for copy in copies:
        copy.wait()


def fused_body(kv_size, tp_size, *args):
    hidden_in, norm_gain, w_query, w_key, w_value, w_out, carried_state = args[:7]
    prior_keys, prior_values, accepted, lengths = args[7:]
    own_rows, width = hidden_in.shape
    block = width // kv_size
    _, head_count, _, key_size = prior_keys.shape
    prior_keys = jnp.transpose(prior_keys, (0, 2, 1, 3))
    prior_values = jnp.transpose(prior_values, (0, 2, 1, 3))
    value_size = prior_values.shape[-1]
    half = key_size // 2
    heads = head_count * tp_size
    per = kv_size // tp_size
    inverse = (rotary_base ** (-np.linspace(0.0, 1.0, half))).astype(np.float32)[None, :]
    decay = (1.0 - 2.0 ** (-5.0 - np.arange(heads))).astype(np.float32)
    bf16, f32 = jnp.bfloat16, jnp.float32
    key_width = head_count * key_size
    value_width = head_count * value_size
    out_width = w_out.shape[0]
    pack_a = own_rows * 2 * key_width // LANE
    pack_b = own_rows * value_width // LANE
    hbm_spec = pl.BlockSpec(memory_space=pltpu.HBM)
    vmem_spec = pl.BlockSpec(memory_space=pltpu.VMEM)
    results = pl.pallas_call(
        functools.partial(layer_kernel, kv_size, tp_size),
        out_shape=(
            pltpu.VMEM((per * own_rows, out_width), bf16),
            pltpu.VMEM(carried_state.shape, f32),
            pltpu.VMEM(prior_keys.shape, bf16),
            pltpu.VMEM(prior_values.shape, bf16),
        ),
        in_specs=[hbm_spec] * 9 + [pl.BlockSpec(memory_space=pltpu.SMEM)] * 2 + [hbm_spec] * 2,
        out_specs=(vmem_spec,) * 4,
        scratch_shapes=[
            pltpu.VMEM(hidden_in.shape, bf16),
            pltpu.VMEM((1, width), f32),
            pltpu.VMEM(w_query.shape, bf16),
            pltpu.VMEM(w_key.shape, bf16),
            pltpu.VMEM(w_value.shape, bf16),
            pltpu.VMEM(w_out.shape, bf16),
            pltpu.VMEM(carried_state.shape[1:], bf16),
            pltpu.VMEM(prior_keys.shape, bf16),
            pltpu.VMEM(prior_values.shape, bf16),
            pltpu.VMEM((1, half), f32),
            pltpu.SMEM((heads,), f32),
            pltpu.VMEM(hidden_in.shape, bf16),
            pltpu.VMEM((kv_size, own_rows, block), bf16),
            pltpu.VMEM((kv_size * SUB, block), f32),
            pltpu.VMEM((kv_size, pack_a, LANE), bf16),
            pltpu.VMEM((kv_size, pack_a, LANE), bf16),
            pltpu.VMEM((kv_size, pack_b, LANE), bf16),
            pltpu.VMEM((kv_size, pack_b, LANE), bf16),
            pltpu.VMEM((kv_size, max(pack_a, pack_b), LANE), f32),
            pltpu.VMEM((pack_a, LANE), f32),
            pltpu.VMEM((pack_b, LANE), f32),
            pltpu.VMEM((kv_size, own_rows, value_width), bf16),
            pltpu.VMEM((kv_size * SUB, value_width), f32),
            pltpu.VMEM((tp_size, per, own_rows, out_width), bf16),
            pltpu.VMEM((tp_size, per, own_rows, out_width), bf16),
            pltpu.VMEM((per * own_rows, out_width), f32),
            pltpu.SemaphoreType.DMA((11,)),
            pltpu.SemaphoreType.DMA((kv_size,)),
            pltpu.SemaphoreType.DMA((kv_size,)),
            pltpu.SemaphoreType.DMA((2, kv_size)),
            pltpu.SemaphoreType.DMA((2, kv_size)),
            pltpu.SemaphoreType.DMA((kv_size,)),
            pltpu.SemaphoreType.DMA((kv_size,)),
            pltpu.SemaphoreType.DMA((tp_size,)),
            pltpu.SemaphoreType.DMA((tp_size,)),
        ],
        compiler_params=pltpu.CompilerParams(collective_id=0, has_side_effects=True),
    )(
        hidden_in,
        norm_gain.reshape(1, width),
        w_query,
        w_key,
        w_value,
        w_out,
        carried_state,
        prior_keys,
        prior_values,
        accepted,
        lengths,
        inverse,
        decay,
    )
    layer_out, committed, new_keys, new_values = pl.pallas_call(
        finish_kernel,
        out_shape=tuple(jax.ShapeDtypeStruct(r.shape, r.dtype) for r in results),
        in_specs=[vmem_spec] * 4,
        out_specs=(hbm_spec,) * 4,
        scratch_shapes=[pltpu.SemaphoreType.DMA((4,))],
    )(*[pltpu.with_memory_space_constraint(r, pltpu.VMEM) for r in results])
    return (
        layer_out,
        committed,
        jnp.transpose(new_keys, (0, 2, 1, 3)),
        jnp.transpose(new_values, (0, 2, 1, 3)),
    )


def kernel_fits(args):
    hidden_in, w_query, w_out, prior_keys = args[0], args[2], args[5], args[7]
    kv_size, tp_size = lax.axis_size("kv"), lax.axis_size("tp")
    return (
        prior_keys.shape[0] == 1
        and hidden_in.shape[0] == prior_keys.shape[2] <= SUB
        and w_query.shape[0] % LANE == 0
        and w_out.shape[0] % LANE == 0
        and prior_keys.shape[3] % (2 * LANE) == 0
        and kv_size % tp_size == 0
    )


def either(*args):
    if kernel_fits(args):
        return fused_body(lax.axis_size("kv"), lax.axis_size("tp"), *args)
    return body(*args)


def solution(mesh):
    in_specs = (
        P("kv", None),
        P(),
        P("kv", "tp"),
        P("kv", "tp"),
        P("kv", "tp"),
        P("kv", "tp"),
        P("kv", "tp", None, None),
        P("kv", "tp", None, None),
        P("kv", "tp", None, None),
        P("kv"),
        P("kv"),
    )
    out_specs = (
        P("tp", "kv"),
        P("kv", "tp", None, None),
        P("kv", "tp", None, None),
        P("kv", "tp", None, None),
    )
    return jax.shard_map(either, mesh=mesh, in_specs=in_specs, out_specs=out_specs, check_vma=False)
```

```python
import functools

import jax
import jax.numpy as jnp
import numpy as np
from jax import lax
from jax.experimental import pallas as pl
from jax.experimental.pallas import tpu as pltpu
from jax.sharding import PartitionSpec as P

epsilon = 1e-06
rotary_base = 10000.0


def rotate(values, places):
    middle = values.shape[-1] // 2
    inverse = rotary_base ** (-jnp.linspace(0.0, 1.0, middle, dtype=jnp.float32))
    angles = places[..., None] * inverse
    cosine = jnp.cos(angles)[:, :, None, :]
    sine_term = jnp.sin(angles)[:, :, None, :]
    leading = values[..., :middle]
    trailing = values[..., middle:]
    return jnp.concatenate(
        [leading * cosine - trailing * sine_term, leading * sine_term + trailing * cosine], axis=-1
    )


def retain(
    queries,
    key_rows,
    value_rows,
    carried_state,
    prior_keys,
    prior_values,
    accepted,
    lengths,
    head_ids,
):
    steps_ahead = queries.shape[1]
    key_size = queries.shape[-1]
    log_decay = jnp.log(1.0 - 2.0 ** (-5.0 - head_ids))
    slot_ids = jnp.arange(steps_ahead, dtype=jnp.float32)
    places = (lengths + accepted).astype(jnp.float32)[:, None] + slot_ids[None, :]
    turned_q = rotate(queries.astype(jnp.float32), places)
    turned_k = rotate(key_rows.astype(jnp.float32), places) * key_size ** (-0.5)
    taken_count = accepted.astype(jnp.float32)[:, None]
    lag_steps = taken_count[:, :, None] - 1.0 - slot_ids[None, None, :]
    weights_back = jnp.where(
        lag_steps >= 0.0, jnp.exp(log_decay[None, :, None] * jnp.maximum(lag_steps, 0.0)), 0.0
    )
    keep_factor = jnp.exp(log_decay[None, :] * taken_count)
    scaled_keys = prior_keys.astype(jnp.float32) * weights_back[..., None]
    committed = keep_factor[..., None, None] * carried_state + jnp.einsum(
        "shjd,shje->shde",
        scaled_keys,
        prior_values.astype(jnp.float32),
        precision=lax.Precision.HIGHEST,
    )
    reach_decay = jnp.exp(log_decay[None, :] * (slot_ids[:, None] + 1.0))
    carried_part = (
        jnp.einsum("sihd,shde->sihe", turned_q, committed, precision=lax.Precision.HIGHEST)
        * reach_decay[None, :, :, None]
    )
    distance = slot_ids[:, None] - slot_ids[None, :]
    weight = jnp.where(
        distance[None] >= 0.0,
        jnp.exp(log_decay[:, None, None] * jnp.maximum(distance, 0.0)[None]),
        0.0,
    )
    scores = (
        jnp.einsum("sihd,sjhd->shij", turned_q, turned_k, precision=lax.Precision.HIGHEST)
        * weight[None]
    )
    inner_part = jnp.einsum(
        "shij,sjhe->sihe", scores, value_rows.astype(jnp.float32), precision=lax.Precision.HIGHEST
    )
    retained = carried_part + inner_part
    normed = retained * lax.rsqrt(jnp.mean(retained * retained, axis=-1, keepdims=True) + epsilon)
    return (normed.astype(jnp.bfloat16), committed, turned_k)


def body(
    hidden_in,
    norm_gain,
    w_query,
    w_key,
    w_value,
    w_out,
    carried_state,
    prior_keys,
    prior_values,
    accepted,
    lengths,
):
    row_values = hidden_in.astype(jnp.float32)
    normed = (
        row_values
        * lax.rsqrt(jnp.mean(row_values * row_values, axis=-1, keepdims=True) + epsilon)
        * norm_gain
    ).astype(jnp.bfloat16)
    own_rows = normed.shape[0]
    query_width = w_query.shape[1]
    key_width = w_key.shape[1]
    columns = lax.all_to_all(normed, "kv", split_axis=1, concat_axis=0, tiled=True)
    joined = jnp.concatenate((w_query, w_key, w_value), axis=1)
    group_count = lax.axis_size("kv")
    partial_term = jnp.dot(columns, joined, preferred_element_type=jnp.float32)
    grouped = partial_term.reshape(group_count, own_rows, partial_term.shape[1])
    received = lax.all_to_all(grouped, "kv", split_axis=0, concat_axis=0, tiled=True)
    joint_sum = jnp.sum(received, axis=0)
    query_sum = joint_sum[:, :query_width]
    key_sum = joint_sum[:, query_width : query_width + key_width]
    value_sum = joint_sum[:, query_width + key_width :]
    seq_count, head_count, steps_ahead = (
        prior_keys.shape[0],
        prior_keys.shape[1],
        prior_keys.shape[2],
    )

    def by_heads(matrix):
        return matrix.astype(jnp.bfloat16).reshape(seq_count, steps_ahead, head_count, -1)

    value_rows = by_heads(value_sum)
    head_ids = (lax.axis_index("tp") * head_count + jnp.arange(head_count)).astype(jnp.float32)
    heads_out, committed, turned_k = retain(
        by_heads(query_sum),
        by_heads(key_sum),
        value_rows,
        carried_state,
        prior_keys,
        prior_values,
        accepted,
        lengths,
        head_ids,
    )
    flat_rows = heads_out.reshape(own_rows, -1)
    head_terms = lax.dot_general(
        lax.all_gather(flat_rows, "kv", axis=0, tiled=True),
        w_out,
        (((1,), (1,)), ((), ())),
        preferred_element_type=jnp.float32,
    )
    layer_out = lax.psum_scatter(
        head_terms.astype(jnp.bfloat16), "tp", scatter_dimension=0, tiled=True
    )
    new_keys = jnp.transpose(turned_k, (0, 2, 1, 3)).astype(jnp.bfloat16)
    new_values = jnp.transpose(value_rows, (0, 2, 1, 3))
    return (layer_out, committed, new_keys, new_values)


MESH_ID = pl.DeviceIdType.MESH
SUB = 8
LANE = 128


def layer_kernel(
    kv_size,
    tp_size,
    hidden_hbm,
    gain_hbm,
    w_query_hbm,
    w_key_hbm,
    w_value_hbm,
    w_out_hbm,
    carried_hbm,
    prior_keys_hbm,
    prior_values_hbm,
    accepted_hbm,
    lengths_hbm,
    inverse_hbm,
    decay_hbm,
    layer_out_ref,
    state,
    own_keys,
    own_values,
    hidden,
    gain,
    w_query,
    w_key,
    w_value,
    w_out,
    state_low,
    prior_keys,
    prior_values,
    inverse,
    decay,
    normed,
    rows_recv,
    rows_pad,
    part_send_a,
    part_recv_a,
    part_send_b,
    part_recv_b,
    packed,
    summed_a,
    summed_b,
    heads_all,
    heads_pad,
    out_send,
    out_recv,
    out_rows,
    load_sems,
    a_send,
    a_recv,
    b_send,
    b_recv,
    c_send,
    c_recv,
    d_send,
    d_recv,
):
    me = lax.axis_index("kv")
    mine = lax.axis_index("tp")
    own_rows, width = hidden.shape
    block = width // kv_size
    head_count, key_size, value_size = state.shape[1:]
    half = key_size // 2
    key_width = head_count * key_size
    value_width = head_count * value_size
    per = kv_size // tp_size

    def kv_peer(d):
        return lax.rem(me + d, kv_size)

    def tp_peer(d):
        return lax.rem(mine + d, tp_size)

    barrier = pltpu.get_barrier_semaphore()
    for d in range(1, kv_size):
        pl.semaphore_signal(barrier, inc=1, device_id={"kv": kv_peer(d)}, device_id_type=MESH_ID)
    for d in range(1, tp_size):
        pl.semaphore_signal(barrier, inc=1, device_id={"tp": tp_peer(d)}, device_id_type=MESH_ID)

    pairs = (
        (hidden_hbm, hidden),
        (gain_hbm, gain),
        (inverse_hbm, inverse),
        (decay_hbm, decay),
        (prior_keys_hbm, prior_keys),
        (prior_values_hbm, prior_values),
        (carried_hbm, state),
        (w_query_hbm, w_query),
        (w_key_hbm, w_key),
        (w_value_hbm, w_value),
        (w_out_hbm, w_out),
    )
    loads = [pltpu.make_async_copy(s, t, load_sems.at[k]) for k, (s, t) in enumerate(pairs)]
    for load in loads:
        load.start()

    order = range(1, kv_size)

    def far_offset(k):
        upper = lax.div(me * 2, kv_size)
        falling = kv_size - k - lax.div(me + k, kv_size)
        rising = k - 1 + lax.div(k - 1 - me + kv_size, kv_size)
        peer = (1 - upper) * falling + upper * rising
        return lax.rem(peer - me + kv_size, kv_size)

    loads[0].wait()
    loads[1].wait()
    row_values = hidden[...].astype(jnp.float32)
    mean = jnp.mean(row_values * row_values, axis=-1, keepdims=True)
    normed[...] = (row_values * lax.rsqrt(mean + epsilon) * gain[...]).astype(jnp.bfloat16)
    rows_pad[...] = jnp.zeros_like(rows_pad)
    heads_pad[...] = jnp.zeros_like(heads_pad)

    pl.semaphore_wait(barrier, kv_size - 1 + tp_size - 1)

    sends = []

    def row_copy(d):
        return pltpu.make_async_remote_copy(
            src_ref=normed.at[:, pl.ds(pl.multiple_of(kv_peer(d) * block, LANE), block)],
            dst_ref=rows_recv.at[d],
            send_sem=a_send.at[d],
            recv_sem=a_recv.at[d],
            device_id={"kv": kv_peer(d)},
            device_id_type=MESH_ID,
        )

    for k in order:
        row_copy(far_offset(k)).start()
    waits_a = {d: row_copy(d) for d in order}
    sends += waits_a.values()

    for load in loads[2:7]:
        load.wait()
    taken = jnp.full((1, 1), accepted_hbm[0], jnp.int32)
    start_place = lengths_hbm[0] + taken
    decays = []
    for h in range(head_count):
        g = decay[mine * head_count + h]
        powers = [jnp.float32(1.0)]
        for _ in range(own_rows):
            powers.append(powers[-1] * g)
        decays.append(powers)

    def power_of(powers, count):
        out = jnp.zeros(count.shape, jnp.float32)
        for n, value in enumerate(powers):
            out = jnp.where(count == n, value, out)
        return out

    for h in range(head_count):
        powers = decays[h]
        keep = power_of(powers, taken)
        keys = prior_keys[0, :, h, :].astype(jnp.float32)
        values = prior_values[0, :, h, :].astype(jnp.float32)
        padded = jnp.concatenate([keys, jnp.zeros((SUB - own_rows, key_size), jnp.float32)], axis=0)
        columns = jnp.transpose(padded)
        total = keep * state[0, h]
        for j in range(own_rows):
            weight = power_of(powers, taken - 1 - j)
            total = total + (columns[:, j : j + 1] * weight) * values[j : j + 1, :]
        state[0, h] = total
        state_low[h] = total.astype(jnp.bfloat16)

    step_ids = lax.broadcasted_iota(jnp.int32, (own_rows, half), 0)
    angles = (step_ids + start_place).astype(jnp.float32) * inverse[...]
    cosine = jnp.cos(angles)
    sine = jnp.sin(angles)

    rows_pad[0:own_rows, :] = normed[:, pl.ds(pl.multiple_of(me * block, LANE), block)].astype(jnp.float32)
    for load in loads[7:10]:
        load.wait()
    for d in order:
        waits_a[d].wait_recv()
        rows_pad[SUB * d : SUB * d + own_rows, :] = rows_recv[d].astype(jnp.float32)
    stacked = rows_pad[...].astype(jnp.bfloat16)

    def pack(part, first):
        for d in range(kv_size):
            for g in range(part.shape[1] // LANE):
                low = (first + g) * own_rows
                packed[d, low : low + own_rows, :] = part[
                    SUB * d : SUB * d + own_rows, g * LANE : (g + 1) * LANE
                ]

    def send_parts(send_ref, recv_ref, chunk):
        def part_copy(e):
            return pltpu.make_async_remote_copy(
                src_ref=send_ref.at[lax.rem(kv_size - e, kv_size)],
                dst_ref=recv_ref.at[e],
                send_sem=b_send.at[chunk, e],
                recv_sem=b_recv.at[chunk, e],
                device_id={"kv": kv_peer(e)},
                device_id_type=MESH_ID,
            )

        for k in order:
            part_copy(far_offset(k)).start()
        return [part_copy(e) for e in order]

    query_part = jnp.dot(stacked, w_query[...], preferred_element_type=jnp.float32)
    key_part = jnp.dot(stacked, w_key[...], preferred_element_type=jnp.float32)
    pack(query_part, 0)
    pack(key_part, key_width // LANE)
    part_send_a[...] = packed[:, : part_send_a.shape[1], :].astype(jnp.bfloat16)
    made_a = send_parts(part_send_a, part_recv_a, 0)
    value_part = jnp.dot(stacked, w_value[...], preferred_element_type=jnp.float32)
    own_a = packed[0, : part_send_a.shape[1], :]
    pack(value_part, 0)
    part_send_b[...] = packed[:, : part_send_b.shape[1], :].astype(jnp.bfloat16)
    made_b = send_parts(part_send_b, part_recv_b, 1)
    sends += made_a + made_b

    joint = own_a
    for copy in made_a:
        copy.wait_recv()
    for d in order:
        joint = joint + part_recv_a[d].astype(jnp.float32)
    summed_a[...] = joint.astype(jnp.bfloat16).astype(jnp.float32)

    def unpack(ref, column, size):
        low = column // LANE
        return jnp.concatenate(
            [ref[g * own_rows : (g + 1) * own_rows, :] for g in range(low, low + size // LANE)], axis=1
        )

    def turn(rows):
        leading = rows[:, :half]
        trailing = rows[:, half:]
        return jnp.concatenate(
            [leading * cosine - trailing * sine, leading * sine + trailing * cosine], axis=1
        )

    row_ids = lax.broadcasted_iota(jnp.int32, (own_rows, 1), 0)
    carried_parts = []
    score_columns = []
    for h in range(head_count):
        powers = decays[h]
        turned_q = turn(unpack(summed_a, h * key_size, key_size))
        turned_k = turn(unpack(summed_a, key_width + h * key_size, key_size))
        turned_k = turned_k * key_size ** (-0.5)
        own_keys[0, :, h, :] = turned_k.astype(jnp.bfloat16)
        reach = jnp.zeros((own_rows, 1), jnp.float32)
        for i in range(own_rows):
            reach = jnp.where(row_ids == i, powers[i + 1], reach)
        carried_parts.append(
            jnp.dot(turned_q.astype(jnp.bfloat16), state_low[h], preferred_element_type=jnp.float32)
            * reach
        )
        columns = []
        for j in range(own_rows):
            weight = jnp.zeros((own_rows, 1), jnp.float32)
            for i in range(j, own_rows):
                weight = jnp.where(row_ids == i, powers[i - j], weight)
            score = jnp.sum(turned_q * turned_k[j : j + 1, :], axis=-1, keepdims=True)
            columns.append(score * weight)
        score_columns.append(columns)

    value_rows = packed[0, : part_send_b.shape[1], :]
    for copy in made_b:
        copy.wait_recv()
    for d in order:
        value_rows = value_rows + part_recv_b[d].astype(jnp.float32)
    summed_b[...] = value_rows.astype(jnp.bfloat16).astype(jnp.float32)
    head_rows = []
    for h in range(head_count):
        values = unpack(summed_b, h * value_size, value_size)
        own_values[0, :, h, :] = values.astype(jnp.bfloat16)
        retained = carried_parts[h]
        for j in range(own_rows):
            retained = retained + score_columns[h][j] * values[j : j + 1, :]
        mean = jnp.mean(retained * retained, axis=-1, keepdims=True)
        head_rows.append(retained * lax.rsqrt(mean + epsilon))
    heads_all[me] = jnp.concatenate(head_rows, axis=1).astype(jnp.bfloat16)

    def head_copy(d):
        return pltpu.make_async_remote_copy(
            src_ref=heads_all.at[me],
            dst_ref=heads_all.at[me],
            send_sem=c_send.at[d],
            recv_sem=c_recv.at[d],
            device_id={"kv": kv_peer(d)},
            device_id_type=MESH_ID,
        )

    for k in order:
        head_copy(far_offset(k)).start()
    sends += [head_copy(d) for d in order]
    loads[10].wait()
    for d in order:
        pltpu.make_async_remote_copy(
            src_ref=heads_all.at[me],
            dst_ref=heads_all.at[kv_peer(kv_size - d)],
            send_sem=c_send.at[d],
            recv_sem=c_recv.at[d],
            device_id={"kv": kv_peer(d)},
            device_id_type=MESH_ID,
        ).wait_recv()
    for j in range(kv_size):
        heads_pad[SUB * j : SUB * j + own_rows, :] = heads_all[j].astype(jnp.float32)
    terms = lax.dot_general(
        heads_pad[...].astype(jnp.bfloat16),
        w_out[...],
        (((1,), (1,)), ((), ())),
        preferred_element_type=jnp.float32,
    )
    for t in range(tp_size):
        for i in range(per):
            j = t * per + i
            out_send[t, i] = terms[SUB * j : SUB * j + own_rows, :].astype(jnp.bfloat16)
    waits_d = []
    for d in range(1, tp_size):
        copy = pltpu.make_async_remote_copy(
            src_ref=out_send.at[tp_peer(d)],
            dst_ref=out_recv.at[d],
            send_sem=d_send.at[d],
            recv_sem=d_recv.at[d],
            device_id={"tp": tp_peer(d)},
            device_id_type=MESH_ID,
        )
        copy.start()
        waits_d.append(copy)
    sends += waits_d
    own_terms = out_send[mine].astype(jnp.float32)
    for copy in waits_d:
        copy.wait_recv()
    for d in range(1, tp_size):
        own_terms = own_terms + out_recv[d].astype(jnp.float32)
    for i in range(per):
        out_rows[own_rows * i : own_rows * (i + 1), :] = own_terms[i]
    layer_out_ref[...] = out_rows[...].astype(jnp.bfloat16)
    for copy in sends:
        copy.wait_send()


def finish_kernel(*refs):
    sources, targets, sems = refs[:4], refs[4:8], refs[8]
    copies = [
        pltpu.make_async_copy(s, t, sems.at[k]) for k, (s, t) in enumerate(zip(sources, targets))
    ]
    for copy in reversed(copies):
        copy.start()
    for copy in copies:
        copy.wait()


def fused_body(kv_size, tp_size, *args):
    hidden_in, norm_gain, w_query, w_key, w_value, w_out, carried_state = args[:7]
    prior_keys, prior_values, accepted, lengths = args[7:]
    own_rows, width = hidden_in.shape
    block = width // kv_size
    _, head_count, _, key_size = prior_keys.shape
    prior_keys = jnp.transpose(prior_keys, (0, 2, 1, 3))
    prior_values = jnp.transpose(prior_values, (0, 2, 1, 3))
    value_size = prior_values.shape[-1]
    half = key_size // 2
    heads = head_count * tp_size
    per = kv_size // tp_size
    inverse = (rotary_base ** (-np.linspace(0.0, 1.0, half))).astype(np.float32)[None, :]
    decay = (1.0 - 2.0 ** (-5.0 - np.arange(heads))).astype(np.float32)
    bf16, f32 = jnp.bfloat16, jnp.float32
    key_width = head_count * key_size
    value_width = head_count * value_size
    out_width = w_out.shape[0]
    pack_a = own_rows * 2 * key_width // LANE
    pack_b = own_rows * value_width // LANE
    hbm_spec = pl.BlockSpec(memory_space=pltpu.HBM)
    vmem_spec = pl.BlockSpec(memory_space=pltpu.VMEM)
    results = pl.pallas_call(
        functools.partial(layer_kernel, kv_size, tp_size),
        out_shape=(
            pltpu.VMEM((per * own_rows, out_width), bf16),
            pltpu.VMEM(carried_state.shape, f32),
            pltpu.VMEM(prior_keys.shape, bf16),
            pltpu.VMEM(prior_values.shape, bf16),
        ),
        in_specs=[hbm_spec] * 9 + [pl.BlockSpec(memory_space=pltpu.SMEM)] * 2 + [hbm_spec] * 2,
        out_specs=(vmem_spec,) * 4,
        scratch_shapes=[
            pltpu.VMEM(hidden_in.shape, bf16),
            pltpu.VMEM((1, width), f32),
            pltpu.VMEM(w_query.shape, bf16),
            pltpu.VMEM(w_key.shape, bf16),
            pltpu.VMEM(w_value.shape, bf16),
            pltpu.VMEM(w_out.shape, bf16),
            pltpu.VMEM(carried_state.shape[1:], bf16),
            pltpu.VMEM(prior_keys.shape, bf16),
            pltpu.VMEM(prior_values.shape, bf16),
            pltpu.VMEM((1, half), f32),
            pltpu.SMEM((heads,), f32),
            pltpu.VMEM(hidden_in.shape, bf16),
            pltpu.VMEM((kv_size, own_rows, block), bf16),
            pltpu.VMEM((kv_size * SUB, block), f32),
            pltpu.VMEM((kv_size, pack_a, LANE), bf16),
            pltpu.VMEM((kv_size, pack_a, LANE), bf16),
            pltpu.VMEM((kv_size, pack_b, LANE), bf16),
            pltpu.VMEM((kv_size, pack_b, LANE), bf16),
            pltpu.VMEM((kv_size, max(pack_a, pack_b), LANE), f32),
            pltpu.VMEM((pack_a, LANE), f32),
            pltpu.VMEM((pack_b, LANE), f32),
            pltpu.VMEM((kv_size, own_rows, value_width), bf16),
            pltpu.VMEM((kv_size * SUB, value_width), f32),
            pltpu.VMEM((tp_size, per, own_rows, out_width), bf16),
            pltpu.VMEM((tp_size, per, own_rows, out_width), bf16),
            pltpu.VMEM((per * own_rows, out_width), f32),
            pltpu.SemaphoreType.DMA((11,)),
            pltpu.SemaphoreType.DMA((kv_size,)),
            pltpu.SemaphoreType.DMA((kv_size,)),
            pltpu.SemaphoreType.DMA((2, kv_size)),
            pltpu.SemaphoreType.DMA((2, kv_size)),
            pltpu.SemaphoreType.DMA((kv_size,)),
            pltpu.SemaphoreType.DMA((kv_size,)),
            pltpu.SemaphoreType.DMA((tp_size,)),
            pltpu.SemaphoreType.DMA((tp_size,)),
        ],
        compiler_params=pltpu.CompilerParams(collective_id=0, has_side_effects=True),
    )(
        hidden_in,
        norm_gain.reshape(1, width),
        w_query,
        w_key,
        w_value,
        w_out,
        carried_state,
        prior_keys,
        prior_values,
        accepted,
        lengths,
        inverse,
        decay,
    )
    layer_out, committed, new_keys, new_values = pl.pallas_call(
        finish_kernel,
        out_shape=tuple(jax.ShapeDtypeStruct(r.shape, r.dtype) for r in results),
        in_specs=[vmem_spec] * 4,
        out_specs=(hbm_spec,) * 4,
        scratch_shapes=[pltpu.SemaphoreType.DMA((4,))],
    )(*[pltpu.with_memory_space_constraint(r, pltpu.VMEM) for r in results])
    return (
        layer_out,
        committed,
        jnp.transpose(new_keys, (0, 2, 1, 3)),
        jnp.transpose(new_values, (0, 2, 1, 3)),
    )


def kernel_fits(args):
    hidden_in, w_query, w_out, prior_keys = args[0], args[2], args[5], args[7]
    kv_size, tp_size = lax.axis_size("kv"), lax.axis_size("tp")
    return (
        prior_keys.shape[0] == 1
        and hidden_in.shape[0] == prior_keys.shape[2] <= SUB
        and w_query.shape[0] % LANE == 0
        and w_out.shape[0] % LANE == 0
        and prior_keys.shape[3] % (2 * LANE) == 0
        and kv_size % tp_size == 0
    )


def either(*args):
    if kernel_fits(args):
        return fused_body(lax.axis_size("kv"), lax.axis_size("tp"), *args)
    return body(*args)


def solution(mesh):
    in_specs = (
        P("kv", None),
        P(),
        P("kv", "tp"),
        P("kv", "tp"),
        P("kv", "tp"),
        P("kv", "tp"),
        P("kv", "tp", None, None),
        P("kv", "tp", None, None),
        P("kv", "tp", None, None),
        P("kv"),
        P("kv"),
    )
    out_specs = (
        P("tp", "kv"),
        P("kv", "tp", None, None),
        P("kv", "tp", None, None),
        P("kv", "tp", None, None),
    )
    return jax.shard_map(either, mesh=mesh, in_specs=in_specs, out_specs=out_specs, check_vma=False)
```
